256 devices in a mesh: ep: 64 (over z, x, core), tp: 4 (over y).
Axes of the slice: x: 4, y: 4, z: 8, core: 2. Of those that a mesh axis runs over, the one named last changes fastest.
Arguments:
- queries: bfloat16 [16384, 1024], P('ep', 'tp'), may hold values from -6 to 6
- key_rows: bfloat16 [16384, 1024], P('ep', 'tp'), may hold values from -6 to 6
- value_rows: bfloat16 [16384, 1024], P('ep', 'tp'), may hold values from -6 to 6
- out_gate: bfloat16 [16384, 1024], P('ep', 'tp'), may hold values from -6 to 6
- log_decay: float32 [16384, 8], P('ep', 'tp'), may hold values from -3 to 0, as said below
- head_gain: float32 [8, 128], P('tp'), may hold values from 0.1 to 1.9
- out_weight: bfloat16 [1024, 2048], P('tp'), may hold values from -0.1875 to 0.1875
- moe_input: bfloat16 [8192, 2048], P('ep'), may hold values from -6 to 6
- moe_gain: float32 [2048], replicated, may hold values from 0.1 to 1.9
- expert_gate: bfloat16 [64, 2048, 3584], P('ep', None, 'tp'), may hold values from -0.125 to 0.125
- expert_up: bfloat16 [64, 2048, 3584], P('ep', None, 'tp'), may hold values from -0.125 to 0.125
- expert_down: bfloat16 [64, 3584, 2048], P('ep', 'tp'), may hold values from -0.125 to 0.125
- route_ids: int32 [8192, 2], P('ep'), may hold values from 0 to 63, all different within a row; in each aligned block of 128 rows (0 to 127, 128 to 255, ...) at most 8 rows name the same one
- route_weights: float32 [8192, 2], P('ep'), may hold values from 0.2 to 1
Outputs:
- mixer_out: bfloat16 [16384, 2048], P(('ep', 'tp'))
- expert_out: bfloat16 [8192, 2048], P('ep', 'tp')
The draws below stay inside these ranges and needn't reach their ends.
Inputs may be any that keep to these rules, and one draw needn't show every extreme that they name: `route_ids`: among the 2 entries of a row no expert repeats. In each aligned block of 128 rows (the rows of one index of ep) no expert is named more than 8 times, a bound that some block reaches. `log_decay`: every entry is negative.
All inputs are finite; a program needn't handle non-finite values.
Results may differ from the reference program's by a relative error of at most 0.017.
Values may be sent and summed in bfloat16 or wider, within the bound.
No kernel may reach another device: no remote copies, remote signals or barrier semaphores. Data moves between devices by JAX's collectives and lax.ppermute only.
A program may use at most 64 MiB of HBM per device.

```python
import math
import jax
import jax.numpy as jnp
import numpy as np
from jax import lax

D = 2048
HEADS = 8
HEAD = 128
EFF = 3584
TOP = 2
TOK_DEV = 256
MOE_TOK = 128
TOKENS = 16384
EXPERTS = 64
CAP = 8
MOE_TOTAL = 8192
N_EP = 64
N_TP = 4


def draw_log_decay(key, part):
    streams = jax.random.split(key, 7)
    ranking = jax.random.permutation(streams[0], HEADS)
    fast_heads = ranking < HEADS // 2
    quick = jnp.exp(jax.random.uniform(streams[1], (HEADS,), jnp.float32, jnp.log(3.0), jnp.log(8.0))) / TOK_DEV
    gentle = jnp.exp(jax.random.uniform(streams[2], (HEADS,), jnp.float32, jnp.log(0.03), jnp.log(0.25))) / TOKENS
    fading_speeds = jnp.where(fast_heads, quick, gentle)
    blocks = TOKENS // TOK_DEV
    multiplier_coefficient = jnp.exp(jax.random.uniform(streams[3], (blocks,), jnp.float32, jnp.log(0.5), jnp.log(2.0)))
    multiplier_coefficient = jnp.repeat(multiplier_coefficient, TOK_DEV)
    approximate_guess = jnp.exp(jax.random.uniform(streams[4], (TOKENS, HEADS), jnp.float32, -0.5, 0.5))
    word_slot_spots = jax.random.randint(streams[5], (2, HEADS), 0, TOKENS)
    stack_level_count = jax.random.uniform(streams[6], (2, HEADS), jnp.float32, jnp.log(0.6), jnp.log(0.85))
    sequence_offsets = jnp.arange(TOKENS, dtype=jnp.int32)[:, None, None]
    spike_clusters = jnp.sum(jnp.where(sequence_offsets == word_slot_spots[None], stack_level_count[None], 0.0), axis=1)
    return -(fading_speeds[None, :] * multiplier_coefficient[:, None] * approximate_guess) + spike_clusters


def raised(values, stream_key, source, target, parts, factor):
    owner, partner = [(jnp.arange(values.shape[position]) // (values.shape[position] // parts)).reshape([-1 if axis == position else 1 for axis in range(values.ndim)]) for position in (source, target)]
    chosen = jax.random.permutation(stream_key, parts)[partner]
    strong = (owner == chosen) | (owner == (partner + parts // 2) % parts)
    return jnp.where(strong, factor * values, values)


def levels(stream_key, shape, cuts, low, high):
    level, own = 1.0, jax.random.fold_in(stream_key, 6)
    for position, parts in cuts:
        draws = jnp.exp(jax.random.uniform(jax.random.fold_in(own, position), (parts,), jnp.float32, low / len(cuts), high / len(cuts)))
        level = level * jnp.repeat(draws, shape[position] // parts).reshape([-1 if axis == position else 1 for axis in range(len(shape))])
    return level


def assign_block(key, own, number, rows, amount, top, bound, lean):
    order = jax.random.permutation(key, amount)
    packed, ordinary = load_shares(amount, rows * top, bound, lean, True), load_shares(amount, rows * top, bound, lean, False)
    places = jnp.arange(amount)

    def named(tallies, rotation):
        used = int((tallies > 0).sum())
        fixed = max(1, used // 4)
        passed = fixed + (places - fixed + rotation * (used - fixed)) % max(1, amount - fixed)
        return jnp.zeros((amount,), jnp.int32).at[order[jnp.where(places < fixed, places, passed)]].set(jnp.asarray(tallies, jnp.int32))

    tallies = jnp.where(number % 4 == 0, named(packed, number // 4), named(ordinary, number - number // 4 - 1))
    mixed = jax.random.permutation(jax.random.fold_in(own, 3), amount)
    source_of, sink = mixed[0:amount // 2 * 2:2], mixed[1:amount // 2 * 2:2]
    room = jnp.minimum(tallies[source_of] - 1, bound - tallies[sink]) // 2
    room = jnp.where((source_of == order[0]) | (sink == order[0]) | (tallies[sink] == 0), 0, jnp.maximum(room, 0))
    passed = jax.random.randint(jax.random.fold_in(own, 4), (amount // 2,), 0, 1 << 20) % (room + 1)
    tallies = tallies.at[source_of].add(-passed).at[sink].add(passed)
    members = jnp.searchsorted(jnp.cumsum(tallies), jnp.arange(rows * top), side="right").astype(jnp.int32)
    table = members.reshape(top, rows).T
    table = table[jax.random.permutation(jax.random.fold_in(own, 1), rows)]
    rotation = jax.random.randint(jax.random.fold_in(own, 2), (rows, 1), 0, top)
    return jnp.take_along_axis(table, (jnp.arange(top)[None, :] + rotation) % top, axis=1)


def load_shares(count, total, most, slope, full):
    loads = [(1 << 20) // math.isqrt(grade ** slope) + 1 for grade in range(1, count + 1)]
    largest = most if full else min(most, max(-(-total // count), total * loads[0] // sum(loads)))
    least = 1 if total - largest >= count - 1 else 0
    holding, rest = [largest] + [least] * (count - 1), total - largest - least * (count - 1)
    while rest > 0:
        free = [i for i in range(1, count) if holding[i] < largest] or [i for i in range(1, count) if holding[i] < most]
        mass, left = sum([loads[i] for i in free]), rest
        for i in free:
            more = min(most - holding[i], max(1, left * loads[i] // mass), rest)
            holding[i] = holding[i] + more
            rest = rest - more
    return np.array(holding)


def noise(key, dims, scale, most, cuts=(), kind=jnp.bfloat16):
    drawn = scale * jax.random.normal(key, dims, jnp.float32)
    if cuts:
        drawn = drawn * levels(key, dims, cuts, -0.22, 0.18)
    return jnp.clip(drawn, -most, most).astype(kind)


def noise_with(own_key, shape, width, most, pieces, heavy, held_as=jnp.bfloat16):
    entries = width * jax.random.normal(own_key, shape, jnp.float32)
    if pieces:
        entries = entries * levels(own_key, shape, pieces, -0.22, 0.18)
    return jnp.clip(raised(entries, jax.random.fold_in(own_key, 3), *heavy), -most, most).astype(held_as)


def setup_inputs(seed: int = 0) -> dict:
    streams_of = jax.random.split(jax.random.key(seed), 15)
    queries = noise(streams_of[0], (TOKENS, HEADS * HEAD), 1.0, 6.0, ((0, 64), (1, 4)))
    key_rows = noise(streams_of[1], (TOKENS, HEADS * HEAD), 1.0, 6.0, ((0, 64), (1, 4)))
    value_rows = noise(streams_of[2], (TOKENS, HEADS * HEAD), 1.0, 6.0, ((0, 64), (1, 4)))
    out_gate = noise(streams_of[3], (TOKENS, HEADS * HEAD), 1.0, 6.0, ((0, 64), (1, 4)))
    log_decay = draw_log_decay(jax.random.fold_in(streams_of[14], 71), 0)
    head_gain = jnp.clip(1.0 + 0.18 * jax.random.normal(streams_of[5], (HEADS, HEAD), jnp.float32), 0.1, 1.9)
    out_weight = noise(streams_of[6], (HEADS * HEAD, D), (HEADS * HEAD) ** -0.5, 0.1875, ((0, 4),))
    moe_input = noise(streams_of[7], (MOE_TOTAL, D), 1.0, 6.0, ((0, 64),))
    moe_gain = jnp.clip(1.0 + 0.18 * jax.random.normal(streams_of[8], (D,), jnp.float32), 0.1, 1.9)
    expert_gate = noise(streams_of[9], (EXPERTS, D, EFF), D ** -0.5, 0.125, ((0, 64), (2, 4)))
    expert_up = noise(streams_of[10], (EXPERTS, D, EFF), D ** -0.5, 0.125, ((0, 64), (2, 4)))
    expert_down = noise_with(streams_of[11], (EXPERTS, EFF, D), EFF ** -0.5, 0.125, ((0, 64), (1, 4)), (1, 2, 4, 2.0))
    route_ids_keys = jax.random.split(jax.random.fold_in(streams_of[12], 1), MOE_TOTAL // MOE_TOK)
    route_ids_turns = jax.random.permutation(jax.random.fold_in(streams_of[12], 3), MOE_TOTAL // MOE_TOK)
    route_ids = jax.vmap(lambda own, number: assign_block(jax.random.fold_in(streams_of[12], 2), own, number, MOE_TOK, EXPERTS, TOP, CAP, 2))(route_ids_keys, route_ids_turns).reshape((MOE_TOTAL, TOP))
    route_weights = jnp.clip(0.2 + 0.8 * jax.random.uniform(streams_of[13], (MOE_TOTAL, TOP), jnp.float32) ** levels(streams_of[13], (MOE_TOTAL, TOP), ((0, 64),), -0.2, 0.2), 0.2, 1.0)
    return {"queries": queries, "key_rows": key_rows, "value_rows": value_rows, "out_gate": out_gate, "log_decay": log_decay, "head_gain": head_gain, "out_weight": out_weight, "moe_input": moe_input, "moe_gain": moe_gain, "expert_gate": expert_gate, "expert_up": expert_up, "expert_down": expert_down, "route_ids": route_ids, "route_weights": route_weights}


epsilon = 1e-06

def retention_block(state, inputs):
    query_heads, key_heads, value_heads, decay_block = inputs
    query_f = query_heads.astype(jnp.float32)
    key_f = key_heads.astype(jnp.float32)
    value_f = value_heads.astype(jnp.float32)
    cumulative = jnp.cumsum(decay_block, axis=0)
    block_total = cumulative[-1]
    scores = jnp.einsum('thd,shd->hts', query_f, key_f) * HEAD ** (-0.5)
    level = cumulative.T
    causal = jnp.arange(TOK_DEV, dtype=jnp.int32)[:, None] >= jnp.arange(TOK_DEV, dtype=jnp.int32)[None, :]
    spread = jnp.where(causal[None], level[:, :, None] - level[:, None, :], -jnp.inf)
    weights = (scores * jnp.exp(spread)).astype(jnp.bfloat16)
    inner = jnp.einsum('hts,shd->thd', weights.astype(jnp.float32), value_f)
    carried = jnp.einsum('thd,hde->the', query_f * jnp.exp(cumulative)[:, :, None], state, precision=lax.Precision.HIGHEST)
    scaled_keys = key_f * jnp.exp(block_total[None, :] - cumulative)[:, :, None]
    fresh = jnp.einsum('thd,the->hde', scaled_keys, value_f, precision=lax.Precision.HIGHEST)
    new_state = jnp.exp(block_total)[:, None, None] * state + fresh
    return (new_state, inner + carried)

def retention_ref(queries, key_rows, value_rows, out_gate, log_decay, head_gain, out_weight):
    blocks = TOKENS // TOK_DEV
    shaped = (blocks, TOK_DEV, HEADS, HEAD)
    start = jnp.zeros((HEADS, HEAD, HEAD), jnp.float32)
    _, retained = lax.scan(retention_block, start, (queries.reshape(shaped), key_rows.reshape(shaped), value_rows.reshape(shaped), log_decay.reshape(blocks, TOK_DEV, HEADS)))
    retained = retained.reshape(TOKENS, HEADS, HEAD)
    normed = retained * lax.rsqrt(lax.optimization_barrier(jnp.mean(retained * retained, axis=-1, keepdims=True)) + epsilon) * head_gain[None]
    gated = normed * jax.nn.silu(out_gate.reshape(TOKENS, HEADS, HEAD).astype(jnp.float32))
    heads_out = gated.reshape(TOKENS, HEADS * HEAD).astype(jnp.bfloat16)
    group = HEADS * HEAD // N_TP
    summed = jnp.zeros((TOKENS, D), jnp.float32)
    for member in range(N_TP):
        partial_sum = jnp.dot(heads_out[:, member * group:(member + 1) * group], out_weight[member * group:(member + 1) * group], preferred_element_type=jnp.float32).astype(jnp.bfloat16)
        summed = summed + lax.optimization_barrier(partial_sum).astype(jnp.float32)
    return summed.astype(jnp.bfloat16)

def slot_targets(block_ids):
    flat_ids = block_ids.reshape(-1)
    member = (flat_ids[:, None] == jnp.arange(EXPERTS, dtype=jnp.int32)[None, :]).astype(jnp.int32)
    ranks = lax.optimization_barrier(jnp.sum(jnp.cumsum(member, axis=0) * member, axis=1)) - 1
    return flat_ids * CAP + ranks

def experts_ref(moe_input, moe_gain, expert_gate, expert_up, expert_down, route_ids, route_weights):
    rows_f = moe_input.astype(jnp.float32)
    normed = (rows_f * lax.rsqrt(lax.optimization_barrier(jnp.mean(rows_f * rows_f, axis=-1, keepdims=True)) + epsilon) * moe_gain[None]).astype(jnp.bfloat16)
    pairs = MOE_TOK * TOP
    targets = jax.vmap(slot_targets)(route_ids.reshape(N_EP, MOE_TOK, TOP))
    pair_weights = route_weights.reshape(N_EP, pairs)
    block_index = jnp.arange(N_EP, dtype=jnp.int32)[:, None]
    group = EFF // N_TP

    def one_expert(total, expert):
        wanted = targets // CAP == expert
        local_slot = jnp.where(wanted, targets % CAP, CAP).astype(jnp.int32)
        table = jnp.full((N_EP, CAP + 1), pairs, jnp.int32)
        table = table.at[block_index, local_slot].set(jnp.arange(pairs, dtype=jnp.int32)[None, :])[:, :CAP]
        filled = table < pairs
        pair_index = jnp.minimum(table, pairs - 1)
        token_index = block_index * MOE_TOK + pair_index // TOP
        rows = jnp.where(filled[:, :, None], normed[token_index], jnp.zeros((), jnp.bfloat16)).reshape(N_EP * CAP, D)
        gate_w = lax.dynamic_index_in_dim(expert_gate, expert, 0, keepdims=False)
        up_w = lax.dynamic_index_in_dim(expert_up, expert, 0, keepdims=False)
        down_w = lax.dynamic_index_in_dim(expert_down, expert, 0, keepdims=False)
        hidden = (jax.nn.silu(jnp.dot(rows, gate_w, preferred_element_type=jnp.float32)) * jnp.dot(rows, up_w, preferred_element_type=jnp.float32)).astype(jnp.bfloat16)
        summed = jnp.zeros((N_EP * CAP, D), jnp.float32)
        for member in range(N_TP):
            partial_sum = jnp.dot(hidden[:, member * group:(member + 1) * group], down_w[member * group:(member + 1) * group], preferred_element_type=jnp.float32).astype(jnp.bfloat16)
            summed = summed + lax.optimization_barrier(partial_sum).astype(jnp.float32)
        results = summed.astype(jnp.bfloat16).astype(jnp.float32)
        scale = jnp.where(filled, jnp.take_along_axis(pair_weights, pair_index, axis=1), 0.0)
        contrib = scale.reshape(-1)[:, None] * results
        total = total.at[token_index.reshape(-1)].add(contrib)
        return (total, None)
    start = jnp.zeros((MOE_TOTAL, D), jnp.float32)
    total, _ = lax.scan(one_expert, start, jnp.arange(EXPERTS, dtype=jnp.int32))
    return total.astype(jnp.bfloat16)

def reference(queries, key_rows, value_rows, out_gate, log_decay, head_gain, out_weight, moe_input, moe_gain, expert_gate, expert_up, expert_down, route_ids, route_weights):
    mixer_out = retention_ref(queries, key_rows, value_rows, out_gate, log_decay, head_gain, out_weight)
    expert_out = experts_ref(moe_input, moe_gain, expert_gate, expert_up, expert_down, route_ids, route_weights)
    return (mixer_out, expert_out)
```

```python
import functools

import jax
import jax.numpy as jnp
from jax import lax
from jax.experimental import pallas as pl
from jax.experimental.pallas import tpu as pltpu
from jax.sharding import Mesh
from jax.sharding import PartitionSpec as P

EP = ("z", "x", "c")
ZX = ("z", "x")
F32 = jnp.float32
BF16 = jnp.bfloat16
epsilon = 1e-06


def iota(shape, dim):
    return lax.broadcasted_iota(jnp.int32, shape, dim)


def dot(a, b):
    return jnp.dot(a, b, preferred_element_type=F32)


def dot_t(a, b):
    return lax.dot_general(a, b, (((0,), (0,)), ((), ())), preferred_element_type=F32)


def three_parts(x):
    a = x.astype(BF16)
    rest = x - a.astype(F32)
    b = rest.astype(BF16)
    return a, b, (rest - b.astype(F32)).astype(BF16)


def call(body, outs, *args, **kw):
    return pl.pallas_call(
        body,
        out_shape=outs,
        in_specs=[pl.BlockSpec(memory_space=pltpu.VMEM)] * len(args),
        out_specs=jax.tree.map(lambda _: pl.BlockSpec(memory_space=pltpu.VMEM), outs),
        **kw,
    )(*args)


def array(shape, dtype):
    return jax.ShapeDtypeStruct(shape, dtype)


def slot_members(ids_ref, half, rows, capacity):
    tokens = ids_ref.shape[0]
    eye = (iota((tokens, tokens), 0) == iota((tokens, tokens), 1)).astype(BF16)
    ids = dot_t(ids_ref[...].astype(F32).astype(BF16), eye).astype(jnp.int32)
    core = lax.axis_index("c")
    slot = iota((rows, 1), 0)
    other = core + half - 2 * core * half
    expert = (slot // capacity) * 2 + other
    first, second = ids[0:1] == expert, ids[1:2] == expert
    member = jnp.where(first | second, 1.0, 0.0)
    earlier = (iota((tokens, tokens), 0) < iota((tokens, tokens), 1)).astype(BF16)
    rank = dot(member.astype(BF16), earlier).astype(jnp.int32)
    here = rank == (slot % capacity)
    return first & here, second & here


def dispatch_kernel(capacity, ids_ref, x_ref, gain_ref, keep_ref, send_ref):
    part = keep_ref.shape[1]
    x = x_ref[...].astype(F32)
    scale = lax.rsqrt(jnp.mean(x * x, axis=-1, keepdims=True) + epsilon)
    cols = pl.ds(pl.multiple_of(lax.axis_index("tp") * part, part), part)
    normed = (x_ref[:, cols].astype(F32) * scale * gain_ref[:, cols]).astype(BF16)
    for half, ref in enumerate((keep_ref, send_ref)):
        first, second = slot_members(ids_ref, half, ref.shape[0], capacity)
        hot = jnp.where(first | second, 1.0, 0.0).astype(BF16)
        ref[...] = dot(hot, normed).astype(BF16)


def blend_weights_kernel(capacity, ids_ref, w_ref, out_ref):
    tokens = ids_ref.shape[0]
    eye = (iota((tokens, tokens), 0) == iota((tokens, tokens), 1)).astype(BF16)
    w = sum(dot_t(t, eye) for t in three_parts(w_ref[...]))
    for half in range(2):
        first, second = slot_members(ids_ref, half, out_ref.shape[2], capacity)
        blend = jnp.where(first, w[0:1], 0.0) + jnp.where(second, w[1:2], 0.0)
        hi = blend.astype(BF16)
        out_ref[half, 0] = hi
        out_ref[half, 1] = (blend - hi.astype(F32)).astype(BF16)


def blend_kernel(w_ref, keep_ref, sent_ref, out_ref):
    total = 0.0
    for half, ref in enumerate((keep_ref, sent_ref)):
        rows = ref[...]
        total = total + dot_t(w_ref[half, 0], rows) + dot_t(w_ref[half, 1], rows)
    out_ref[...] = total.astype(BF16)


def ffn_kernel(own, left, right, far_a, far_b, gate, up, down, to2a, to2b, to1a, to1b, tom1a, tom1b, mine):
    me = lax.axis_index("tp")
    part = own.shape[1]
    half = far_a.shape[0]
    hidden = gate.shape[1]
    far = jnp.concatenate([far_a[...], far_b[...]], axis=0)

    def span(k):
        return pl.ds(pl.multiple_of(lax.rem(me + k, 4) * part, part), part)

    pieces = ((0, own[...]), (3, left[...]), (1, right[...]), (2, far))
    hid = []
    for lo in range(0, hidden, 256):
        hi = min(hidden, lo + 256)
        g = sum(dot(x, gate[span(k), lo:hi]) for k, x in pieces)
        u = sum(dot(x, up[span(k), lo:hi]) for k, x in pieces)
        hid.append((g * jax.nn.sigmoid(g) * u).astype(BF16))
    hid = jnp.concatenate(hid, axis=1)
    for k, (top, low) in ((2, (to2a, to2b)), (1, (to1a, to1b)), (3, (tom1a, tom1b)), (0, (None, None))):
        out = dot(hid, down[:, span(k)]).astype(BF16)
        if k == 0:
            mine[...] = out
        else:
            top[...] = out[:half]
            low[...] = out[half:]


def levels_of(decay):
    n = decay.shape[0]
    parts = jnp.concatenate(three_parts(decay), axis=1)
    upto = (iota((n, n), 0) >= iota((n, n), 1)).astype(BF16)
    before = (iota((n, n), 0) <= iota((n, n), 1)).astype(BF16)
    col = dot(upto, parts)
    row = dot_t(parts, before)
    return col[:, 0:2] + col[:, 2:4] + col[:, 4:6], row[0:2] + row[2:4] + row[4:6]


def inner_kernel(q_ref, k_ref, v_ref, decay_ref, inner_ref, kept_ref, kept_total_ref, send_ref):
    core = lax.axis_index("c")
    n = q_ref.shape[0]
    col, row = levels_of(decay_ref[...])
    causal = iota((n, n), 0) >= iota((n, n), 1)
    states, totals = [], []
    for h in range(2):
        cols = slice(h * 128, h * 128 + 128)
        q, k, v = q_ref[:, cols], k_ref[:, cols], v_ref[:, cols]
        scores = lax.dot_general(q, k, (((1,), (1,)), ((), ())), preferred_element_type=F32) * 128 ** (-0.5)
        spread = jnp.where(causal, col[:, h : h + 1] - row[h : h + 1], -jnp.inf)
        inner_ref[:, cols] = dot((scores * jnp.exp(spread)).astype(BF16), v)
        total = col[n - 1 : n, h : h + 1]
        scaled = (k.astype(F32) * jnp.exp(total - col[:, h : h + 1])).astype(BF16)
        states.append(dot_t(scaled, v))
        totals.append(total)
    first = core == 0
    kept_ref[...] = jnp.where(first, states[0], states[1])
    kept_total_ref[...] = jnp.broadcast_to(jnp.where(first, totals[0], totals[1]), kept_total_ref.shape)
    send_ref[0:128] = jnp.where(first, states[1], states[0]).astype(BF16)
    send_ref[128:144] = rows_of_total(jnp.where(first, totals[1], totals[0]), 16)


def rows_of_total(total, rows):
    a, b, c = (jnp.broadcast_to(t.astype(F32), (rows, 128)) for t in three_parts(total))
    r = iota((rows, 128), 0)
    return jnp.where(r == 0, a, jnp.where(r == 1, b, jnp.where(r == 2, c, 0.0))).astype(BF16)


def pair_of(kept_ref, kept_total_ref, got_ref):
    first = lax.axis_index("c") == 0
    mine, mine_total = kept_ref[...], kept_total_ref[0:1]
    theirs = got_ref[0:128].astype(F32)
    rows = got_ref[128:144].astype(F32)
    theirs_total = rows[0:1] + rows[1:2] + rows[2:3]
    return (
        (jnp.where(first, mine, theirs), jnp.where(first, mine_total, theirs_total)),
        (jnp.where(first, theirs, mine), jnp.where(first, theirs_total, mine_total)),
    )


def pair_kernel(kept_ref, kept_total_ref, got_ref, out_ref):
    (s0, t0), (s1, t1) = pair_of(kept_ref, kept_total_ref, got_ref)
    state = (jnp.exp(t1) * s0 + s1).astype(BF16)
    total = rows_of_total(t0 + t1, 4)
    for j in range(out_ref.shape[0]):
        out_ref[j, 0:4] = state[4 * j : 4 * j + 4]
        out_ref[j, 4:8] = total


def scan_kernel(in_ref, out_ref):
    state = jnp.zeros((4, 128), F32)
    for j in range(in_ref.shape[0]):
        hi = state.astype(BF16)
        out_ref[j, 0:4] = hi
        out_ref[j, 4:8] = (state - hi.astype(F32)).astype(BF16)
        block = in_ref[j].astype(F32)
        state = jnp.exp(block[4:5] + block[5:6] + block[6:7]) * state + block[0:4]


def entering_kernel(back_ref, kept_ref, kept_total_ref, got_ref, keep_ref, send_ref):
    (s0, t0), _ = pair_of(kept_ref, kept_total_ref, got_ref)
    rows = []
    for j in range(back_ref.shape[0]):
        block = back_ref[j].astype(F32)
        rows.append(block[0:4] + block[4:8])
    before = jnp.concatenate(rows, axis=0)
    after = jnp.exp(t0) * before + s0
    first = lax.axis_index("c") == 0
    keep_ref[...] = jnp.where(first, before, after).astype(BF16)
    send_ref[...] = jnp.where(first, after, before).astype(BF16)


def mixer_kernel(inner_ref, q_ref, decay_ref, keep_ref, got_ref, gain_ref, gate_ref, weight_ref, out_ref):
    first = lax.axis_index("c") == 0
    col, _ = levels_of(decay_ref[...])
    keep, got = keep_ref[...], got_ref[...]
    entering = (jnp.where(first, keep, got), jnp.where(first, got, keep))
    heads = []
    for h in range(2):
        cols = slice(h * 128, h * 128 + 128)
        carried = jnp.exp(col[:, h : h + 1]) * dot(q_ref[:, cols], entering[h])
        kept = inner_ref[:, cols] + carried
        normed = kept * lax.rsqrt(jnp.mean(kept * kept, axis=-1, keepdims=True) + epsilon) * gain_ref[h : h + 1]
        gate = gate_ref[:, cols].astype(F32)
        heads.append((normed * (gate * jax.nn.sigmoid(gate))).astype(BF16))
    heads = jnp.concatenate(heads, axis=1)
    for lo in range(0, out_ref.shape[1], 512):
        out_ref[:, lo : lo + 512] = dot(heads, weight_ref[:, lo : lo + 512]).astype(BF16)


def shifted(x, axis, by):
    n = lax.axis_size(axis)
    return lax.ppermute(x, axis, [(i, (i + by) % n) for i in range(n)])


def across_chips(x):
    n = lax.axis_size(ZX)
    out = lax.all_to_all(x.reshape(n, -1, x.shape[-1]), ZX, split_axis=0, concat_axis=0, tiled=True)
    return out.reshape(x.shape)


def gathered(x):
    half = x.shape[0] // 2
    left, right = shifted(x, "tp", 1), shifted(x, "tp", -1)
    far_a, far_b = shifted(left[:half], "tp", 1), shifted(right[half:], "tp", -1)
    return x, left, right, far_a, far_b


def reduced(to2a, to2b, to1a, to1b, tom1a, tom1b, mine):
    def add(*parts):
        return sum(p.astype(F32) for p in parts).astype(BF16)

    half = to2a.shape[0]
    a, b = shifted(to2a, "tp", 1), shifted(to2b, "tp", -1)
    l_low, r_top = shifted(to1b, "tp", 1), shifted(tom1a, "tp", -1)
    l_top, r_low = shifted(add(to1a, a), "tp", 1), shifted(add(tom1b, b), "tp", -1)
    return jnp.concatenate([add(mine[:half], l_top, r_top), add(mine[half:], l_low, r_low)], axis=0)


def per_device(
    queries,
    key_rows,
    value_rows,
    out_gate,
    log_decay,
    head_gain,
    out_weight,
    moe_input,
    moe_gain,
    expert_gate,
    expert_up,
    expert_down,
    route_ids,
    route_weights,
):
    tokens, width = moe_input.shape
    part = width // lax.axis_size("tp")
    chips = lax.axis_size(ZX)
    capacity = 2 * route_ids.size // lax.axis_size(EP)
    rows = chips * capacity
    half = rows // 2
    keep, send = call(
        functools.partial(dispatch_kernel, capacity),
        [array((rows, part), BF16)] * 2,
        route_ids,
        moe_input,
        moe_gain.reshape(1, -1),
        name="dispatch",
    )
    got = shifted(send, "c", 1)
    arrived = across_chips(keep), across_chips(got)

    inner, kept, kept_total, state_send = call(
        inner_kernel,
        [array(queries.shape, F32), array((128, 128), F32), array((8, 128), F32), array((144, 128), BF16)],
        queries,
        key_rows,
        value_rows,
        log_decay,
        name="inner",
    )
    state_got = shifted(state_send, "c", 1)
    pair = call(pair_kernel, array((chips, 8, 128), BF16), kept, kept_total, state_got, name="pair")
    scanned = call(scan_kernel, array((chips, 8, 128), BF16), across_chips(pair.reshape(-1, 128)).reshape(pair.shape), name="scan")
    back = across_chips(scanned.reshape(-1, 128)).reshape(pair.shape)
    ent_keep, ent_send = call(
        entering_kernel, [array((128, 128), BF16)] * 2, back, kept, kept_total, state_got, name="entering"
    )
    ent_got = shifted(ent_send, "c", 1)
    partial = call(
        mixer_kernel,
        array((queries.shape[0], out_weight.shape[1]), BF16),
        inner,
        queries,
        log_decay,
        ent_keep,
        ent_got,
        head_gain,
        out_gate,
        out_weight,
        name="mixer",
    )

    results = []
    for chunk in arrived:
        outs = call(
            ffn_kernel,
            [array((half, part), BF16)] * 6 + [array((rows, part), BF16)],
            *gathered(chunk),
            expert_gate[0],
            expert_up[0],
            expert_down[0],
            name="ffn",
        )
        results.append(across_chips(reduced(*outs)))
    weights = call(
        functools.partial(blend_weights_kernel, capacity),
        array((2, 2, rows, tokens), BF16),
        route_ids,
        route_weights,
        name="blend_weights",
    )
    expert_out = call(
        blend_kernel, array((tokens, part), BF16), weights, results[0], shifted(results[1], "c", 1), name="blend"
    )
    pieces = lax.all_to_all(partial.reshape(4, -1, partial.shape[1]), "tp", 0, 0, tiled=True)
    mixer_out = jnp.sum(pieces.astype(F32), axis=0).astype(BF16)
    return mixer_out, expert_out


def solution(mesh):
    split = Mesh(mesh.devices.reshape(8, 4, 2, mesh.shape["tp"]), ("z", "x", "c", "tp"))
    return jax.shard_map(
        per_device,
        mesh=split,
        in_specs=(
            P(EP, "tp"),
            P(EP, "tp"),
            P(EP, "tp"),
            P(EP, "tp"),
            P(EP, "tp"),
            P("tp", None),
            P("tp", None),
            P(EP, None),
            P(),
            P(EP, None, "tp"),
            P(EP, None, "tp"),
            P(EP, "tp", None),
            P(EP, None),
            P(EP, None),
        ),
        out_specs=(P((*EP, "tp"), None), P(EP, "tp")),
        check_vma=False,
    )
```

```python
import functools

import jax
import jax.numpy as jnp
from jax import lax
from jax.experimental import pallas as pl
from jax.experimental.pallas import tpu as pltpu
from jax.sharding import Mesh
from jax.sharding import PartitionSpec as P


EP = ("z", "x", "c")
ZX = ("z", "x")
F32 = jnp.float32
BF16 = jnp.bfloat16
epsilon = 1e-06
VMEM_LIMIT = 16 << 20


def iota(shape, dim):
    return lax.broadcasted_iota(jnp.int32, shape, dim)


def dot(a, b):
    return jnp.dot(a, b, preferred_element_type=F32)


def dot_t(a, b):
    return lax.dot_general(a, b, (((0,), (0,)), ((), ())), preferred_element_type=F32)


def three_parts(x):
    a = x.astype(BF16)
    rest = x - a.astype(F32)
    b = rest.astype(BF16)
    return a, b, (rest - b.astype(F32)).astype(BF16)


def call(body, outs, *args, plain=0, held=(), scratch_shapes=(), limit=VMEM_LIMIT):
    space = pl.BlockSpec(memory_space=pltpu.VMEM)
    kernel = pl.pallas_call(
        body,
        out_shape=outs,
        in_specs=[pl.BlockSpec(memory_space=pl.ANY)] * len(held) + [space] * len(args),
        out_specs=[space] * len(outs) if isinstance(outs, list) else space,
        scratch_shapes=scratch_shapes,
        compiler_params=pltpu.CompilerParams(vmem_limit_bytes=limit),
    )
    hbm = [pltpu.with_memory_space_constraint(a, pltpu.HBM) for a in (*held, *args[:plain])]
    return kernel(*hbm, *(pltpu.with_memory_space_constraint(a, pltpu.VMEM) for a in args[plain:]))


def array(shape, dtype):
    return pltpu.VMEM(shape, dtype)


def slot_members(ids_ref, half, rows, capacity):
    tokens = ids_ref.shape[1]
    core = lax.axis_index("c")
    slot = iota((rows, 1), 0)
    expert = (slot // capacity) * 2 + (core + half - 2 * core * half)
    first, second = ids_ref[0:1] == expert, ids_ref[1:2] == expert
    member = jnp.where(first | second, 1.0, 0.0)
    earlier = (iota((tokens, tokens), 0) < iota((tokens, tokens), 1)).astype(BF16)
    here = dot(member.astype(BF16), earlier).astype(jnp.int32) == slot % capacity
    return first & here, second & here


def dispatch_kernel(capacity, ids_ref, x_ref, gain_ref, keep_ref, send_ref):
    part = keep_ref.shape[1]
    x = x_ref[...].astype(F32)
    scale = lax.rsqrt(jnp.mean(x * x, axis=-1, keepdims=True) + epsilon)
    cols = pl.ds(pl.multiple_of(lax.axis_index("tp") * part, part), part)
    normed = (x_ref[:, cols].astype(F32) * scale * gain_ref[:, cols]).astype(BF16)
    for half, ref in enumerate((keep_ref, send_ref)):
        first, second = slot_members(ids_ref, half, ref.shape[0], capacity)
        hot = jnp.where(first | second, 1.0, 0.0).astype(BF16)
        ref[...] = dot(hot, normed).astype(BF16)


def blend_weights_kernel(capacity, ids_ref, w_ref, out_ref):
    for half in range(2):
        first, second = slot_members(ids_ref, half, out_ref.shape[2], capacity)
        blend = jnp.where(first, w_ref[0:1], 0.0) + jnp.where(second, w_ref[1:2], 0.0)
        hi = blend.astype(BF16)
        out_ref[half, 0] = hi
        out_ref[half, 1] = (blend - hi.astype(F32)).astype(BF16)


def blend_kernel(w_ref, back_ref, sent_ref, out_ref):
    keep = jnp.concatenate([back_ref[j, 0:8] for j in range(back_ref.shape[0])], axis=0)
    total = 0.0
    for half, rows in enumerate((keep, sent_ref[...])):
        total = total + dot_t(w_ref[half, 0], rows) + dot_t(w_ref[half, 1], rows)
    out_ref[...] = total.astype(BF16)


def parted_kernel(back_ref, out_ref):
    for j in range(back_ref.shape[0]):
        out_ref[8 * j : 8 * j + 8] = back_ref[j, 8:16]


def span(k, size):
    n = lax.axis_size("tp")
    return pl.ds(pl.multiple_of(lax.rem(lax.axis_index("tp") + k, n) * size, size), size)


def tiles(size):
    return [slice(lo, min(size, lo + 256)) for lo in range(0, size, 256)]


def started(sems, *pairs):
    copies = [pltpu.make_async_copy(src, dst, sems.at[i]) for i, (src, dst) in enumerate(pairs)]
    for copy in copies:
        copy.start()
    return copies


def near_kernel(gate, up, down, own, left_a, left_b, right_a, right_b, g_ref, u_ref, far_gate, far_up, far_down, gates, ups, sems):
    part = own.shape[1]
    left = (left_a, left_b)
    right = (right_a, right_b)
    order = ((0, (own,)), (3, left), (1, right))
    copies = started(
        sems,
        *(
            pair
            for i, (k, _) in enumerate(order)
            for pair in ((gate.at[span(k, part)], gates.at[i]), (up.at[span(k, part)], ups.at[i]))
        ),
        (gate.at[span(2, part)], far_gate),
        (up.at[span(2, part)], far_up),
        (down.at[:, span(2, part)], far_down),
    )
    for i, (_, refs) in enumerate(order):
        x = jnp.concatenate([r[...] for r in refs], axis=0)
        for weights, total, copy in ((gates, g_ref, copies[2 * i]), (ups, u_ref, copies[2 * i + 1])):
            copy.wait()
            for cols in tiles(total.shape[1]):
                new = dot(x, weights[i, :, cols])
                total[:, cols] = new if i == 0 else total[:, cols] + new
    for copy in copies[6:]:
        copy.wait()


def far_kernel(far_a, far_b, g_in, u_in, gate, up, down, hid_ref, to2a, to2b):
    half = far_a.shape[0]
    far = jnp.concatenate([far_a[...], far_b[...]], axis=0)
    for cols in tiles(gate.shape[1]):
        g = g_in[:, cols] + dot(far, gate[:, cols])
        u = u_in[:, cols] + dot(far, up[:, cols])
        hid_ref[:, cols] = (g * jax.nn.sigmoid(g) * u).astype(BF16)
    out = dot(hid_ref[...], down[...]).astype(BF16)
    to2a[...] = out[:half]
    to2b[...] = out[half:]


def rest_kernel(down, hid, to1a, to1b, tom1a, tom1b, mine, downs, sems):
    part, half = to1a.shape[1], to1a.shape[0]
    order = (1, 3, 0)
    copies = started(sems, *((down.at[:, span(k, part)], downs.at[i]) for i, k in enumerate(order)))
    for i, pair in enumerate(((to1a, to1b), (tom1a, tom1b), (mine.at[:half], mine.at[half:]))):
        copies[i].wait()
        out = dot(hid[...], downs[i]).astype(BF16)
        for ref, rows in zip(pair, (out[:half], out[half:])):
            ref[...] = rows


def onward_kernel(to1a, tom1b, got_a, got_b, out1, outm1):
    out1[...] = (to1a[...].astype(F32) + got_a[...].astype(F32)).astype(BF16)
    outm1[...] = (tom1b[...].astype(F32) + got_b[...].astype(F32)).astype(BF16)


def settle_kernel(mine, top_l, low_l, top_r, low_r, out):
    half = top_l.shape[0]
    for rows, a, b in ((slice(0, half), top_l, top_r), (slice(half, 2 * half), low_l, low_r)):
        out[rows] = (mine[rows].astype(F32) + a[...].astype(F32) + b[...].astype(F32)).astype(BF16)


def join_kernel(keep_ref, got_ref, out_ref):
    for j in range(out_ref.shape[0]):
        out_ref[j, 0:8] = keep_ref[8 * j : 8 * j + 8]
        out_ref[j, 8:16] = got_ref[8 * j : 8 * j + 8]


def levels_of(decay):
    n = decay.shape[1]
    parts = jnp.concatenate([t.astype(F32) for t in three_parts(decay)], axis=0).astype(BF16)
    upto = (iota((n, n), 0) >= iota((n, n), 1)).astype(BF16)
    before = (iota((n, n), 0) <= iota((n, n), 1)).astype(BF16)
    col = lax.dot_general(upto, parts, (((1,), (1,)), ((), ())), preferred_element_type=F32)
    row = dot(parts, before)
    return col[:, 0:2] + col[:, 2:4] + col[:, 4:6], row[0:2] + row[2:4] + row[4:6]


def inner_kernel(q_ref, k_ref, v_ref, decay_ref, inner_ref, kept_ref, kept_total_ref, send_ref):
    core = lax.axis_index("c")
    n = q_ref.shape[0]
    col, row = levels_of(decay_ref[...])
    causal = iota((n, n), 0) >= iota((n, n), 1)
    states, totals = [], []
    for h in range(2):
        cols = slice(h * 128, h * 128 + 128)
        q, k, v = q_ref[:, cols], k_ref[:, cols], v_ref[:, cols]
        scores = lax.dot_general(q, k, (((1,), (1,)), ((), ())), preferred_element_type=F32) * 128 ** (-0.5)
        spread = jnp.where(causal, col[:, h : h + 1] - row[h : h + 1], -jnp.inf)
        inner_ref[:, cols] = dot((scores * jnp.exp(spread)).astype(BF16), v)
        total = col[n - 1 : n, h : h + 1]
        scaled = (k.astype(F32) * jnp.exp(total - col[:, h : h + 1])).astype(BF16)
        states.append(dot_t(scaled, v))
        totals.append(total)
    first = core == 0
    kept_ref[...] = jnp.where(first, states[0], states[1])
    kept_total_ref[...] = jnp.broadcast_to(jnp.where(first, totals[0], totals[1]), kept_total_ref.shape)
    send_ref[0:128] = jnp.where(first, states[1], states[0]).astype(BF16)
    send_ref[128:144] = rows_of_total(jnp.where(first, totals[1], totals[0]), 16)


def rows_of_total(total, rows):
    a, b, c = (jnp.broadcast_to(t.astype(F32), (rows, 128)) for t in three_parts(total))
    r = iota((rows, 128), 0)
    return jnp.where(r == 0, a, jnp.where(r == 1, b, jnp.where(r == 2, c, 0.0))).astype(BF16)


def pair_of(kept_ref, kept_total_ref, got_ref):
    first = lax.axis_index("c") == 0
    mine, mine_total = kept_ref[...], kept_total_ref[0:1]
    theirs = got_ref[0:128].astype(F32)
    rows = got_ref[128:144].astype(F32)
    theirs_total = rows[0:1] + rows[1:2] + rows[2:3]
    return (
        (jnp.where(first, mine, theirs), jnp.where(first, mine_total, theirs_total)),
        (jnp.where(first, theirs, mine), jnp.where(first, theirs_total, mine_total)),
    )


def packed(state, total, out_ref):
    out_ref[0:128] = state.astype(BF16)
    out_ref[128:144] = rows_of_total(total, 16)


def unpacked(ref):
    rows = ref[128:144].astype(F32)
    return ref[0:128].astype(F32), rows[0:1] + rows[1:2] + rows[2:3]


def after(earlier, later):
    return jnp.exp(later[1]) * earlier[0] + later[0], earlier[1] + later[1]


def pair_kernel(kept_ref, kept_total_ref, got_ref, out_ref):
    packed(*after(*pair_of(kept_ref, kept_total_ref, got_ref)), out_ref)


def row_kernel(own_ref, one_ref, two_ref, three_ref, before_ref, before_total_ref, out_ref):
    me = lax.axis_index("x")
    pieces = [unpacked(r) for r in (own_ref, one_ref, two_ref, three_ref)]
    so_far = before = (jnp.zeros((128, 128), F32), jnp.zeros((1, 128), F32))
    for k in range(len(pieces)):
        before = tuple(jnp.where(me == k, new, old) for new, old in zip(so_far, before))
        back = lax.rem(me - k + len(pieces), len(pieces))
        here = pieces[0]
        for by in range(1, len(pieces)):
            here = tuple(jnp.where(back == by, new, old) for new, old in zip(pieces[by], here))
        so_far = after(so_far, here)
    before_ref[...] = before[0]
    before_total_ref[...] = jnp.broadcast_to(before[1], before_total_ref.shape)
    packed(*so_far, out_ref)


def two_kernel(own_ref, one_ref, out_ref):
    packed(*after(unpacked(one_ref), unpacked(own_ref)), out_ref)


def four_kernel(own_ref, one_ref, two_ref, before_ref, before_total_ref, out_ref):
    before = after(unpacked(two_ref), unpacked(one_ref))
    before_ref[...] = before[0]
    before_total_ref[...] = jnp.broadcast_to(before[1], before_total_ref.shape)
    packed(*after(before, unpacked(own_ref)), out_ref)


def entering_kernel(
    four_ref, rows_ref, rows_total_ref, row_ref, row_total_ref, kept_ref, kept_total_ref, got_ref, keep_ref, send_ref
):
    rows, row = (rows_ref[...], rows_total_ref[0:1]), (row_ref[...], row_total_ref[0:1])
    before = after(after(unpacked(four_ref), rows), row)
    later, _ = after(before, pair_of(kept_ref, kept_total_ref, got_ref)[0])
    first = lax.axis_index("c") == 0
    keep_ref[...] = jnp.where(first, before[0], later).astype(BF16)
    send_ref[...] = jnp.where(first, later, before[0]).astype(BF16)


def mixer_kernel(q_ref, decay_ref, gain_ref, gate_ref, weight_ref, inner_ref, keep_ref, got_ref, *refs):
    *outs, rows_ref = refs
    first = lax.axis_index("c") == 0
    col, _ = levels_of(decay_ref[...])
    keep, got = keep_ref[...], got_ref[...]
    entering = (jnp.where(first, keep, got), jnp.where(first, got, keep))
    heads = []
    for h in range(2):
        cols = slice(h * 128, h * 128 + 128)
        carried = jnp.exp(col[:, h : h + 1]) * dot(q_ref[:, cols], entering[h])
        kept = inner_ref[:, cols] + carried
        normed = kept * lax.rsqrt(jnp.mean(kept * kept, axis=-1, keepdims=True) + epsilon) * gain_ref[h : h + 1]
        gate = gate_ref[:, cols].astype(F32)
        heads.append((normed * (gate * jax.nn.sigmoid(gate))).astype(BF16).astype(F32))
    rows_ref[...] = jnp.concatenate(heads, axis=1)
    part = outs[0].shape[0]
    rows = jnp.concatenate([rows_ref[span(k, part)] for k in range(len(outs))], axis=0)
    for lo in range(0, weight_ref.shape[1], 512):
        out = dot(rows.astype(BF16), weight_ref[:, lo : lo + 512]).astype(BF16)
        for k, ref in enumerate(outs):
            ref[:, lo : lo + 512] = out[k * part : (k + 1) * part]


def mix_sum_kernel(mine, right, far, left, out):
    out[...] = sum(r[...].astype(F32) for r in (mine, right, far, left)).astype(BF16)


def shifted(x, axis, by):
    n = lax.axis_size(axis)
    return lax.ppermute(x, axis, [(i, (i + by) % n) for i in range(n)])


def brought(x, axis, by):
    return lax.ppermute(x, axis, [(i, i + by) for i in range(lax.axis_size(axis) - by)])


def across_chips(x):
    n = lax.axis_size(ZX)
    out = lax.all_to_all(x.reshape(n, -1, x.shape[-1]), ZX, split_axis=0, concat_axis=0, tiled=True)
    return out.reshape(x.shape)


def experts(rows, gate, up, down):
    half, part = rows.shape[0] // 2, rows.shape[1]
    hidden = gate.shape[1]
    piece, sums = array((half, part), BF16), [array((2 * half, hidden), F32)] * 2
    top, low = rows[:half], rows[half:]
    left_a, right_b = shifted(top, "tp", 1), shifted(low, "tp", -1)
    left_b, right_a = shifted(low, "tp", 1), shifted(top, "tp", -1)
    far_a, far_b = shifted(left_a, "tp", 1), shifted(right_b, "tp", -1)
    rows_of, cols_of = (part, hidden), (hidden, part)
    g, u, far_gate, far_up, far_down = call(
        near_kernel,
        sums + [array(rows_of, BF16)] * 2 + [array(cols_of, BF16)],
        rows,
        left_a,
        left_b,
        right_a,
        right_b,
        held=(gate, up, down),
        scratch_shapes=[pltpu.VMEM((3, *rows_of), BF16)] * 2 + [pltpu.SemaphoreType.DMA((9,))],
    )
    hid, to2a, to2b = call(
        far_kernel, [array((2 * half, hidden), BF16), piece, piece], far_a, far_b, g, u, far_gate, far_up, far_down
    )
    got_a, got_b = shifted(to2a, "tp", 1), shifted(to2b, "tp", -1)
    to1a, to1b, tom1a, tom1b, mine = call(
        rest_kernel,
        [piece] * 4 + [array((2 * half, part), BF16)],
        hid,
        held=(down,),
        scratch_shapes=[pltpu.VMEM((3, *cols_of), BF16), pltpu.SemaphoreType.DMA((3,))],
    )
    low_l, top_r = shifted(to1b, "tp", 1), shifted(tom1a, "tp", -1)
    to1a, tom1b = call(onward_kernel, [piece] * 2, to1a, tom1b, got_a, got_b)
    top_l, low_r = shifted(to1a, "tp", 1), shifted(tom1b, "tp", -1)
    return call(settle_kernel, array(rows.shape, BF16), mine, top_l, low_l, top_r, low_r)


def per_device(
    queries,
    key_rows,
    value_rows,
    out_gate,
    log_decay,
    head_gain,
    out_weight,
    moe_input,
    moe_gain,
    expert_gate,
    expert_up,
    expert_down,
    route_ids,
    route_weights,
):
    return layer(
        queries,
        key_rows,
        value_rows,
        out_gate,
        log_decay.T,
        head_gain,
        out_weight,
        moe_input,
        moe_gain.reshape(1, -1),
        expert_gate[0],
        expert_up[0],
        expert_down[0],
        route_ids.T,
        route_weights.T,
    )


def layer(q, k, v, out_gate, decay, head_gain, out_weight, x, gain, gate, up, down, ids, blend):
    tokens, width = x.shape
    part = width // lax.axis_size("tp")
    chips = lax.axis_size(ZX)
    capacity = 2 * ids.size // lax.axis_size(EP)
    rows = chips * capacity
    keep, send = call(
        functools.partial(dispatch_kernel, capacity), [array((rows, part), BF16)] * 2, ids, x, gain, plain=3
    )
    got = shifted(send, "c", 1)
    joined = call(join_kernel, array((chips, 2 * capacity, part), BF16), keep, got)
    arrived = across_chips(joined.reshape(-1, part))
    inner, kept, kept_total, state_send = call(
        inner_kernel,
        [array(q.shape, F32), array((128, 128), F32), array((8, 128), F32), array((144, 128), BF16)],
        q,
        k,
        v,
        decay,
        plain=4,
    )
    state_got = shifted(state_send, "c", 1)
    whole, state, total = array((144, 128), BF16), array((128, 128), F32), array((8, 128), F32)
    pair = call(pair_kernel, whole, kept, kept_total, state_got)
    around = [shifted(pair, "x", by) for by in (1, 2, 3)]
    row_before, row_total, row = call(row_kernel, [state, total, whole], pair, *around)
    one = brought(row, "z", 1)
    two = brought(call(two_kernel, whole, row, one), "z", 2)
    rows_before, rows_total, upto = call(four_kernel, [state, total, whole], row, one, two)
    ent_keep, ent_send = call(
        entering_kernel,
        [array((128, 128), BF16)] * 2,
        brought(upto, "z", 4),
        rows_before,
        rows_total,
        row_before,
        row_total,
        kept,
        kept_total,
        state_got,
    )
    ent_got = shifted(ent_send, "c", 1)
    mine, right, far, left = call(
        mixer_kernel,
        [array((q.shape[0] // 4, out_weight.shape[1]), BF16)] * 4,
        q,
        decay,
        head_gain,
        out_gate,
        out_weight,
        inner,
        ent_keep,
        ent_got,
        plain=5,
        scratch_shapes=[pltpu.VMEM(q.shape, F32)],
    )
    mixer_out = call(
        mix_sum_kernel,
        jax.ShapeDtypeStruct(mine.shape, BF16),
        mine,
        shifted(right, "tp", 1),
        shifted(far, "tp", 2),
        shifted(left, "tp", 3),
    )
    weights = call(
        functools.partial(blend_weights_kernel, capacity), array((2, 2, rows, tokens), BF16), ids, blend, plain=2
    )
    results = experts(arrived, gate, up, down)
    back = across_chips(results).reshape(chips, 2 * capacity, part)
    sent = call(parted_kernel, array((rows, part), BF16), back)
    expert_out = call(blend_kernel, jax.ShapeDtypeStruct((tokens, part), BF16), weights, back, shifted(sent, "c", 1))
    return mixer_out, expert_out


def solution(mesh):
    split = Mesh(mesh.devices.reshape(8, 4, 2, mesh.shape["tp"]), ("z", "x", "c", "tp"))
    return jax.shard_map(
        per_device,
        mesh=split,
        in_specs=(
            P(EP, "tp"),
            P(EP, "tp"),
            P(EP, "tp"),
            P(EP, "tp"),
            P(EP, "tp"),
            P("tp", None),
            P("tp", None),
            P(EP, None),
            P(),
            P(EP, None, "tp"),
            P(EP, None, "tp"),
            P(EP, "tp", None),
            P(EP, None),
            P(EP, None),
        ),
        out_specs=(P((*EP, "tp"), None), P(EP, "tp")),
        check_vma=False,
    )
```

```python
import functools

import jax
import jax.numpy as jnp
from jax import lax
from jax.experimental import pallas as pl
from jax.experimental.pallas import tpu as pltpu
from jax.sharding import Mesh
from jax.sharding import PartitionSpec as P


EP = ("z", "x", "c")
ZX = ("z", "x")
F32 = jnp.float32
BF16 = jnp.bfloat16
epsilon = 1e-06
VMEM_LIMIT = 16 << 20


def iota(shape, dim):
    return lax.broadcasted_iota(jnp.int32, shape, dim)


def dot(a, b):
    return jnp.dot(a, b, preferred_element_type=F32)


def dot_t(a, b):
    return lax.dot_general(a, b, (((0,), (0,)), ((), ())), preferred_element_type=F32)


def three_parts(x):
    a = x.astype(BF16)
    rest = x - a.astype(F32)
    b = rest.astype(BF16)
    return a, b, (rest - b.astype(F32)).astype(BF16)


def call(body, outs, *args, plain=0, held=(), scratch_shapes=(), limit=VMEM_LIMIT):
    space = pl.BlockSpec(memory_space=pltpu.VMEM)
    kernel = pl.pallas_call(
        body,
        out_shape=outs,
        in_specs=[pl.BlockSpec(memory_space=pl.ANY)] * len(held) + [space] * len(args),
        out_specs=[space] * len(outs) if isinstance(outs, list) else space,
        scratch_shapes=scratch_shapes,
        compiler_params=pltpu.CompilerParams(vmem_limit_bytes=limit),
    )
    hbm = [pltpu.with_memory_space_constraint(a, pltpu.HBM) for a in (*held, *args[:plain])]
    return kernel(*hbm, *(pltpu.with_memory_space_constraint(a, pltpu.VMEM) for a in args[plain:]))


def array(shape, dtype):
    return pltpu.VMEM(shape, dtype)


def slot_members(ids_ref, half, rows, capacity):
    tokens = ids_ref.shape[1]
    core = lax.axis_index("c")
    slot = iota((rows, 1), 0)
    expert = (slot // capacity) * 2 + (core + half - 2 * core * half)
    first, second = ids_ref[0:1] == expert, ids_ref[1:2] == expert
    member = jnp.where(first | second, 1.0, 0.0)
    earlier = (iota((tokens, tokens), 0) < iota((tokens, tokens), 1)).astype(BF16)
    here = dot(member.astype(BF16), earlier).astype(jnp.int32) == slot % capacity
    return first & here, second & here


def dispatch_kernel(capacity, ids_ref, x_ref, gain_ref, keep_ref, send_ref):
    part = keep_ref.shape[1]
    x = x_ref[...].astype(F32)
    scale = lax.rsqrt(jnp.mean(x * x, axis=-1, keepdims=True) + epsilon)
    cols = pl.ds(pl.multiple_of(lax.axis_index("tp") * part, part), part)
    normed = (x_ref[:, cols].astype(F32) * scale * gain_ref[:, cols]).astype(BF16)
    for half, ref in enumerate((keep_ref, send_ref)):
        first, second = slot_members(ids_ref, half, ref.shape[0], capacity)
        hot = jnp.where(first | second, 1.0, 0.0).astype(BF16)
        ref[...] = dot(hot, normed).astype(BF16)


def blend_weights_kernel(capacity, ids_ref, w_ref, out_ref):
    for half in range(2):
        first, second = slot_members(ids_ref, half, out_ref.shape[2], capacity)
        blend = jnp.where(first, w_ref[0:1], 0.0) + jnp.where(second, w_ref[1:2], 0.0)
        hi = blend.astype(BF16)
        out_ref[half, 0] = hi
        out_ref[half, 1] = (blend - hi.astype(F32)).astype(BF16)


def blend_kernel(w_ref, back_ref, sent_ref, out_ref):
    keep = jnp.concatenate([back_ref[j, 0:8] for j in range(back_ref.shape[0])], axis=0)
    total = 0.0
    for half, rows in enumerate((keep, sent_ref[...])):
        total = total + dot_t(w_ref[half, 0], rows) + dot_t(w_ref[half, 1], rows)
    out_ref[...] = total.astype(BF16)


def parted_kernel(back_ref, out_ref):
    for j in range(back_ref.shape[0]):
        out_ref[8 * j : 8 * j + 8] = back_ref[j, 8:16]


def span(k, size):
    n = lax.axis_size("tp")
    return pl.ds(pl.multiple_of(lax.rem(lax.axis_index("tp") + k, n) * size, size), size)


def tiles(size):
    return [slice(lo, min(size, lo + 256)) for lo in range(0, size, 256)]


def started(sems, *pairs):
    copies = [pltpu.make_async_copy(src, dst, sems.at[i]) for i, (src, dst) in enumerate(pairs)]
    for copy in copies:
        copy.start()
    return copies


def near_kernel(gate, up, down, own, left_a, left_b, right_a, right_b, g_ref, u_ref, far_gate, far_up, far_down, rest_down, gates, ups, sems):
    part = own.shape[1]
    left = (left_a, left_b)
    right = (right_a, right_b)
    order = ((0, (own,)), (3, left), (1, right))
    copies = started(
        sems,
        *(
            pair
            for i, (k, _) in enumerate(order)
            for pair in ((gate.at[span(k, part)], gates.at[i]), (up.at[span(k, part)], ups.at[i]))
        ),
        (gate.at[span(2, part)], far_gate),
        (up.at[span(2, part)], far_up),
        (down.at[:, span(2, part)], far_down),
        *((down.at[:, span(k, part)], rest_down.at[i]) for i, k in enumerate((1, 3, 0))),
    )
    for i, (_, refs) in enumerate(order):
        x = jnp.concatenate([r[...] for r in refs], axis=0)
        for weights, total, copy in ((gates, g_ref, copies[2 * i]), (ups, u_ref, copies[2 * i + 1])):
            copy.wait()
            for cols in tiles(total.shape[1]):
                new = dot(x, weights[i, :, cols])
                total[:, cols] = new if i == 0 else total[:, cols] + new
    for copy in copies[6:]:
        copy.wait()


def far_kernel(far_a, far_b, g_in, u_in, gate, up, down, hid_ref, to2a, to2b):
    half = far_a.shape[0]
    far = jnp.concatenate([far_a[...], far_b[...]], axis=0)
    for cols in tiles(gate.shape[1]):
        g = g_in[:, cols] + dot(far, gate[:, cols])
        u = u_in[:, cols] + dot(far, up[:, cols])
        hid_ref[:, cols] = (g * jax.nn.sigmoid(g) * u).astype(BF16)
    out = dot(hid_ref[...], down[...]).astype(BF16)
    to2a[...] = out[:half]
    to2b[...] = out[half:]


def rest_kernel(hid, down, to1a, to1b, tom1a, tom1b, mine):
    half = to1a.shape[0]
    for i, pair in enumerate(((to1a, to1b), (tom1a, tom1b), (mine.at[:half], mine.at[half:]))):
        out = dot(hid[...], down[i]).astype(BF16)
        for ref, rows in zip(pair, (out[:half], out[half:])):
            ref[...] = rows


def onward_kernel(to1a, tom1b, got_a, got_b, out1, outm1):
    out1[...] = (to1a[...].astype(F32) + got_a[...].astype(F32)).astype(BF16)
    outm1[...] = (tom1b[...].astype(F32) + got_b[...].astype(F32)).astype(BF16)


def settle_kernel(mine, top_l, low_l, top_r, low_r, out):
    half = top_l.shape[0]
    for rows, a, b in ((slice(0, half), top_l, top_r), (slice(half, 2 * half), low_l, low_r)):
        out[rows] = (mine[rows].astype(F32) + a[...].astype(F32) + b[...].astype(F32)).astype(BF16)


def join_kernel(keep_ref, got_ref, out_ref):
    for j in range(out_ref.shape[0]):
        out_ref[j, 0:8] = keep_ref[8 * j : 8 * j + 8]
        out_ref[j, 8:16] = got_ref[8 * j : 8 * j + 8]


def levels_of(decay):
    n = decay.shape[1]
    parts = jnp.concatenate([t.astype(F32) for t in three_parts(decay)], axis=0).astype(BF16)
    upto = (iota((n, n), 0) >= iota((n, n), 1)).astype(BF16)
    before = (iota((n, n), 0) <= iota((n, n), 1)).astype(BF16)
    col = lax.dot_general(upto, parts, (((1,), (1,)), ((), ())), preferred_element_type=F32)
    row = dot(parts, before)
    return col[:, 0:2] + col[:, 2:4] + col[:, 4:6], row[0:2] + row[2:4] + row[4:6]


def inner_kernel(q_ref, k_ref, v_ref, decay_ref, inner_ref, state_ref, total_ref, send_ref):
    n = q_ref.shape[0]
    col, row = levels_of(decay_ref[...])
    causal = iota((n, n), 0) >= iota((n, n), 1)
    for h in range(2):
        cols = slice(h * 128, h * 128 + 128)
        q, k, v = q_ref[:, cols], k_ref[:, cols], v_ref[:, cols]
        scores = lax.dot_general(q, k, (((1,), (1,)), ((), ())), preferred_element_type=F32) * 128 ** (-0.5)
        spread = jnp.where(causal, col[:, h : h + 1] - row[h : h + 1], -jnp.inf)
        inner_ref[:, cols] = dot((scores * jnp.exp(spread)).astype(BF16), v)
        total = col[n - 1 : n, h : h + 1]
        scaled = (k.astype(F32) * jnp.exp(total - col[:, h : h + 1])).astype(BF16)
        state = dot_t(scaled, v)
        kept(h, (state, total), state_ref, total_ref)
        packed(h, (state, total), send_ref)


def rows_of_total(total, rows):
    a, b, c = (jnp.broadcast_to(t.astype(F32), (rows, 128)) for t in three_parts(total))
    r = iota((rows, 128), 0)
    return jnp.where(r == 0, a, jnp.where(r == 1, b, jnp.where(r == 2, c, 0.0))).astype(BF16)


def kept(h, run, state_ref, total_ref):
    state_ref[128 * h : 128 * h + 128] = run[0]
    total_ref[8 * h : 8 * h + 8] = jnp.broadcast_to(run[1], (8, 128))


def had(h, state_ref, total_ref):
    return state_ref[128 * h : 128 * h + 128], total_ref[8 * h : 8 * h + 1]


def packed(h, run, ref):
    ref[144 * h : 144 * h + 128] = run[0].astype(BF16)
    ref[144 * h + 128 : 144 * h + 144] = rows_of_total(run[1], 16)


def unpacked(h, ref):
    rows = ref[144 * h + 128 : 144 * h + 144].astype(F32)
    return ref[144 * h : 144 * h + 128].astype(F32), rows[0:1] + rows[1:2] + rows[2:3]


def after(earlier, later):
    return jnp.exp(later[1]) * earlier[0] + later[0], earlier[1] + later[1]


def chosen(which, a, b):
    return tuple(jnp.where(which, x, y) for x, y in zip(a, b))


def pair_kernel(state_ref, total_ref, got_ref, out_ref):
    first = lax.axis_index("c") == 0
    for h in range(2):
        mine, theirs = had(h, state_ref, total_ref), unpacked(h, got_ref)
        packed(h, after(chosen(first, mine, theirs), chosen(first, theirs, mine)), out_ref)


def row_kernel(own_ref, one_ref, two_ref, three_ref, before_ref, before_total_ref, out_ref):
    me = lax.axis_index("x")
    for h in range(2):
        pieces = [unpacked(h, r) for r in (own_ref, one_ref, two_ref, three_ref)]
        so_far = before = (jnp.zeros((128, 128), F32), jnp.zeros((1, 128), F32))
        for k in range(len(pieces)):
            before = chosen(me == k, so_far, before)
            back = lax.rem(me - k + len(pieces), len(pieces))
            here = pieces[0]
            for by in range(1, len(pieces)):
                here = chosen(back == by, pieces[by], here)
            so_far = after(so_far, here)
        kept(h, before, before_ref, before_total_ref)
        packed(h, so_far, out_ref)


def two_kernel(own_ref, one_ref, out_ref):
    for h in range(2):
        packed(h, after(unpacked(h, one_ref), unpacked(h, own_ref)), out_ref)


def four_kernel(own_ref, one_ref, two_ref, before_ref, before_total_ref, out_ref):
    for h in range(2):
        before = after(unpacked(h, two_ref), unpacked(h, one_ref))
        kept(h, before, before_ref, before_total_ref)
        packed(h, after(before, unpacked(h, own_ref)), out_ref)


def entering(h, four_ref, rows_ref, rows_total_ref, row_ref, row_total_ref, got_ref):
    before = after(after(unpacked(h, four_ref), had(h, rows_ref, rows_total_ref)), had(h, row_ref, row_total_ref))
    later = after(before, unpacked(h, got_ref))
    return jnp.where(lax.axis_index("c") == 0, before[0], later[0]).astype(BF16)


def mixer_kernel(q_ref, decay_ref, gain_ref, gate_ref, weight_ref, inner_ref, *refs):
    *refs, out_0, out_1, out_2, out_3, rows_ref = refs
    outs = (out_0, out_1, out_2, out_3)
    col, _ = levels_of(decay_ref[...])
    heads = []
    for h in range(2):
        cols = slice(h * 128, h * 128 + 128)
        carried = jnp.exp(col[:, h : h + 1]) * dot(q_ref[:, cols], entering(h, *refs))
        whole = inner_ref[:, cols] + carried
        normed = whole * lax.rsqrt(jnp.mean(whole * whole, axis=-1, keepdims=True) + epsilon) * gain_ref[h : h + 1]
        gate = gate_ref[:, cols].astype(F32)
        heads.append((normed * (gate * jax.nn.sigmoid(gate))).astype(BF16).astype(F32))
    rows_ref[...] = jnp.concatenate(heads, axis=1)
    part = outs[0].shape[0]
    rows = jnp.concatenate([rows_ref[span(k, part)] for k in range(len(outs))], axis=0)
    for lo in range(0, weight_ref.shape[1], 512):
        out = dot(rows.astype(BF16), weight_ref[:, lo : lo + 512]).astype(BF16)
        for k, ref in enumerate(outs):
            ref[:, lo : lo + 512] = out[k * part : (k + 1) * part]


def mix_sum_kernel(mine, right, far, left, out):
    out[...] = sum(r[...].astype(F32) for r in (mine, right, far, left)).astype(BF16)


def shifted(x, axis, by):
    n = lax.axis_size(axis)
    return lax.ppermute(x, axis, [(i, (i + by) % n) for i in range(n)])


def brought(x, axis, by):
    return lax.ppermute(x, axis, [(i, i + by) for i in range(lax.axis_size(axis) - by)])


def across_chips(x):
    n = lax.axis_size(ZX)
    out = lax.all_to_all(x.reshape(n, -1, x.shape[-1]), ZX, split_axis=0, concat_axis=0, tiled=True)
    return out.reshape(x.shape)


def experts(rows, gate, up, down):
    half, part = rows.shape[0] // 2, rows.shape[1]
    hidden = gate.shape[1]
    piece, sums = array((half, part), BF16), [array((2 * half, hidden), F32)] * 2
    top, low = rows[:half], rows[half:]
    left_a, right_b = shifted(top, "tp", 1), shifted(low, "tp", -1)
    left_b, right_a = shifted(low, "tp", 1), shifted(top, "tp", -1)
    far_a, far_b = shifted(left_a, "tp", 1), shifted(right_b, "tp", -1)
    rows_of, cols_of = (part, hidden), (hidden, part)
    g, u, far_gate, far_up, far_down, rest_down = call(
        near_kernel,
        sums + [array(rows_of, BF16)] * 2 + [array(cols_of, BF16), array((3, *cols_of), BF16)],
        rows,
        left_a,
        left_b,
        right_a,
        right_b,
        held=(gate, up, down),
        scratch_shapes=[pltpu.VMEM((3, *rows_of), BF16)] * 2 + [pltpu.SemaphoreType.DMA((12,))],
    )
    hid, to2a, to2b = call(
        far_kernel, [array((2 * half, hidden), BF16), piece, piece], far_a, far_b, g, u, far_gate, far_up, far_down
    )
    got_a, got_b = shifted(to2a, "tp", 1), shifted(to2b, "tp", -1)
    to1a, to1b, tom1a, tom1b, mine = call(rest_kernel, [piece] * 4 + [array((2 * half, part), BF16)], hid, rest_down)
    low_l, top_r = shifted(to1b, "tp", 1), shifted(tom1a, "tp", -1)
    to1a, tom1b = call(onward_kernel, [piece] * 2, to1a, tom1b, got_a, got_b)
    top_l, low_r = shifted(to1a, "tp", 1), shifted(tom1b, "tp", -1)
    return call(settle_kernel, array(rows.shape, BF16), mine, top_l, low_l, top_r, low_r)


def per_device(
    queries,
    key_rows,
    value_rows,
    out_gate,
    log_decay,
    head_gain,
    out_weight,
    moe_input,
    moe_gain,
    expert_gate,
    expert_up,
    expert_down,
    route_ids,
    route_weights,
):
    return layer(
        queries,
        key_rows,
        value_rows,
        out_gate,
        log_decay.T,
        head_gain,
        out_weight,
        moe_input,
        moe_gain.reshape(1, -1),
        expert_gate[0],
        expert_up[0],
        expert_down[0],
        route_ids.T,
        route_weights.T,
    )


def layer(q, k, v, out_gate, decay, head_gain, out_weight, x, gain, gate, up, down, ids, blend):
    tokens, width = x.shape
    part = width // lax.axis_size("tp")
    chips = lax.axis_size(ZX)
    capacity = 2 * ids.size // lax.axis_size(EP)
    rows = chips * capacity
    keep, send = call(
        functools.partial(dispatch_kernel, capacity), [array((rows, part), BF16)] * 2, ids, x, gain, plain=3
    )
    got = shifted(send, "c", 1)
    joined = call(join_kernel, array((chips, 2 * capacity, part), BF16), keep, got)
    arrived = across_chips(joined.reshape(-1, part))
    whole, state, total = array((288, 128), BF16), array((256, 128), F32), array((16, 128), F32)
    inner, own_state, own_total, state_send = call(
        inner_kernel, [array(q.shape, F32), state, total, whole], q, k, v, decay, plain=4
    )
    state_got = shifted(state_send, "c", 1)
    pair = call(pair_kernel, whole, own_state, own_total, state_got)
    around = [shifted(pair, "x", by) for by in (1, 2, 3)]
    row_before, row_total, row = call(row_kernel, [state, total, whole], pair, *around)
    one = brought(row, "z", 1)
    two = brought(call(two_kernel, whole, row, one), "z", 2)
    rows_before, rows_total, upto = call(four_kernel, [state, total, whole], row, one, two)
    mine, right, far, left = call(
        mixer_kernel,
        [array((q.shape[0] // 4, out_weight.shape[1]), BF16)] * 4,
        q,
        decay,
        head_gain,
        out_gate,
        out_weight,
        inner,
        brought(upto, "z", 4),
        rows_before,
        rows_total,
        row_before,
        row_total,
        state_got,
        plain=5,
        scratch_shapes=[pltpu.VMEM(q.shape, F32)],
    )
    mixer_out = call(
        mix_sum_kernel,
        jax.ShapeDtypeStruct(mine.shape, BF16),
        mine,
        shifted(right, "tp", 1),
        shifted(far, "tp", 2),
        shifted(left, "tp", 3),
    )
    weights = call(
        functools.partial(blend_weights_kernel, capacity), array((2, 2, rows, tokens), BF16), ids, blend, plain=2
    )
    results = experts(arrived, gate, up, down)
    back = across_chips(results).reshape(chips, 2 * capacity, part)
    sent = call(parted_kernel, array((rows, part), BF16), back)
    expert_out = call(blend_kernel, jax.ShapeDtypeStruct((tokens, part), BF16), weights, back, shifted(sent, "c", 1))
    return mixer_out, expert_out


def solution(mesh):
    split = Mesh(mesh.devices.reshape(8, 4, 2, mesh.shape["tp"]), ("z", "x", "c", "tp"))
    return jax.shard_map(
        per_device,
        mesh=split,
        in_specs=(
            P(EP, "tp"),
            P(EP, "tp"),
            P(EP, "tp"),
            P(EP, "tp"),
            P(EP, "tp"),
            P("tp", None),
            P("tp", None),
            P(EP, None),
            P(),
            P(EP, None, "tp"),
            P(EP, None, "tp"),
            P(EP, "tp", None),
            P(EP, None),
            P(EP, None),
        ),
        out_specs=(P((*EP, "tp"), None), P(EP, "tp")),
        check_vma=False,
    )
```

```python
import functools

import jax
import jax.numpy as jnp
from jax import lax
from jax.experimental import pallas as pl
from jax.experimental.pallas import tpu as pltpu
from jax.sharding import Mesh
from jax.sharding import PartitionSpec as P


EP = ("z", "x", "c")
ZX = ("z", "x")
F32 = jnp.float32
BF16 = jnp.bfloat16
epsilon = 1e-06
VMEM_LIMIT = 16 << 20


def iota(shape, dim):
    return lax.broadcasted_iota(jnp.int32, shape, dim)


def dot(a, b):
    return jnp.dot(a, b, preferred_element_type=F32)


def dot_t(a, b):
    return lax.dot_general(a, b, (((0,), (0,)), ((), ())), preferred_element_type=F32)


def three_parts(x):
    a = x.astype(BF16)
    rest = x - a.astype(F32)
    b = rest.astype(BF16)
    return a, b, (rest - b.astype(F32)).astype(BF16)


def call(body, outs, *args, plain=0, loose=0, held=(), scratch_shapes=()):
    space = pl.BlockSpec(memory_space=pltpu.VMEM)
    kernel = pl.pallas_call(
        body,
        out_shape=outs,
        in_specs=[pl.BlockSpec(memory_space=pl.ANY)] * len(held) + [space] * len(args),
        out_specs=[space] * len(outs) if isinstance(outs, list) else space,
        scratch_shapes=scratch_shapes,
        compiler_params=pltpu.CompilerParams(vmem_limit_bytes=VMEM_LIMIT),
    )
    hbm = [pltpu.with_memory_space_constraint(a, pltpu.HBM) for a in (*held, *args[:plain])]
    rest = (pltpu.with_memory_space_constraint(a, pltpu.VMEM) for a in args[plain + loose :])
    return kernel(*hbm, *args[plain : plain + loose], *rest)


def array(shape, dtype):
    return pltpu.VMEM(shape, dtype)


def slot_members(ids_ref, half, rows, capacity):
    tokens = ids_ref.shape[1]
    core = lax.axis_index("c")
    slot = iota((rows, 1), 0)
    expert = (slot // capacity) * 2 + (core + half - 2 * core * half)
    first, second = ids_ref[0:1] == expert, ids_ref[1:2] == expert
    member = jnp.where(first | second, 1.0, 0.0)
    earlier = (iota((tokens, tokens), 0) < iota((tokens, tokens), 1)).astype(BF16)
    here = dot(member.astype(BF16), earlier).astype(jnp.int32) == slot % capacity
    return first & here, second & here


def dispatch_kernel(capacity, ids_ref, x_ref, gain_ref, keep_ref, send_ref):
    part = keep_ref.shape[1]
    x = x_ref[...].astype(F32)
    scale = lax.rsqrt(jnp.mean(x * x, axis=-1, keepdims=True) + epsilon)
    cols = pl.ds(pl.multiple_of(lax.axis_index("tp") * part, part), part)
    normed = (x_ref[:, cols].astype(F32) * scale * gain_ref[:, cols]).astype(BF16)
    for half, ref in enumerate((keep_ref, send_ref)):
        first, second = slot_members(ids_ref, half, ref.shape[0], capacity)
        hot = jnp.where(first | second, 1.0, 0.0).astype(BF16)
        ref[...] = dot(hot, normed).astype(BF16)


def blend_weights_kernel(capacity, ids_ref, w_ref, out_ref):
    for half in range(2):
        first, second = slot_members(ids_ref, half, out_ref.shape[2], capacity)
        blend = jnp.where(first, w_ref[0:1], 0.0) + jnp.where(second, w_ref[1:2], 0.0)
        hi = blend.astype(BF16)
        out_ref[half, 0] = hi
        out_ref[half, 1] = (blend - hi.astype(F32)).astype(BF16)


def blended(w_ref, half, rows):
    return dot_t(w_ref[half, 0], rows) + dot_t(w_ref[half, 1], rows)


def kept_blend_kernel(w_ref, back_ref, out_ref):
    keep = jnp.concatenate([back_ref[j, 0:8] for j in range(back_ref.shape[0])], axis=0)
    out_ref[...] = blended(w_ref, 0, keep)


def blend_kernel(w_ref, kept_ref, sent_ref, out_ref):
    out_ref[...] = (kept_ref[...] + blended(w_ref, 1, sent_ref[...])).astype(BF16)


def parted_kernel(back_ref, out_ref):
    for j in range(back_ref.shape[0]):
        out_ref[8 * j : 8 * j + 8] = back_ref[j, 8:16]


def span(k, size):
    n = lax.axis_size("tp")
    return pl.ds(pl.multiple_of(lax.rem(lax.axis_index("tp") + k, n) * size, size), size)


def tiles(size):
    return [slice(lo, min(size, lo + 256)) for lo in range(0, size, 256)]


def started(sems, *pairs):
    copies = [pltpu.make_async_copy(src, dst, sems.at[i]) for i, (src, dst) in enumerate(pairs)]
    for copy in copies:
        copy.start()
    return copies


def near_kernel(gate, up, down, own, left_a, left_b, right_a, right_b, g_ref, u_ref, far_gate, far_up, far_down, rest_down, gates, ups, sems):
    part = own.shape[1]
    left = (left_a, left_b)
    right = (right_a, right_b)
    order = ((0, (own,)), (3, left), (1, right))
    copies = started(
        sems,
        *(
            pair
            for i, (k, _) in enumerate(order)
            for pair in ((gate.at[span(k, part)], gates.at[i]), (up.at[span(k, part)], ups.at[i]))
        ),
        (gate.at[span(2, part)], far_gate),
        (up.at[span(2, part)], far_up),
        (down.at[:, span(2, part)], far_down),
        *((down.at[:, span(k, part)], rest_down.at[i]) for i, k in enumerate((1, 3, 0))),
    )
    for i, (_, refs) in enumerate(order):
        x = jnp.concatenate([r[...] for r in refs], axis=0)
        for weights, total, copy in ((gates, g_ref, copies[2 * i]), (ups, u_ref, copies[2 * i + 1])):
            copy.wait()
            for cols in tiles(total.shape[1]):
                new = dot(x, weights[i, :, cols])
                total[:, cols] = new if i == 0 else total[:, cols] + new
    for copy in copies[6:]:
        copy.wait()


def far_kernel(far_a, far_b, g_in, u_in, gate, up, down, hid_ref, to2a, to2b):
    half = far_a.shape[0]
    far = jnp.concatenate([far_a[...], far_b[...]], axis=0)
    for cols in tiles(gate.shape[1]):
        g = g_in[:, cols] + dot(far, gate[:, cols])
        u = u_in[:, cols] + dot(far, up[:, cols])
        hid_ref[:, cols] = (g * jax.nn.sigmoid(g) * u).astype(BF16)
    out = dot(hid_ref[...], down[...]).astype(BF16)
    to2a[...] = out[:half]
    to2b[...] = out[half:]


def rest_kernel(hid, down, to1a, to1b, tom1a, tom1b, mine):
    half = to1a.shape[0]
    for i, pair in enumerate(((to1a, to1b), (tom1a, tom1b), (mine.at[:half], mine.at[half:]))):
        out = dot(hid[...], down[i]).astype(BF16)
        for ref, rows in zip(pair, (out[:half], out[half:])):
            ref[...] = rows


def onward_kernel(to1a, tom1b, got_a, got_b, out1, outm1):
    out1[...] = (to1a[...].astype(F32) + got_a[...].astype(F32)).astype(BF16)
    outm1[...] = (tom1b[...].astype(F32) + got_b[...].astype(F32)).astype(BF16)


def settle_kernel(mine, top_l, low_l, top_r, low_r, out):
    half = top_l.shape[0]
    for rows, a, b in ((slice(0, half), top_l, top_r), (slice(half, 2 * half), low_l, low_r)):
        out[rows] = (mine[rows].astype(F32) + a[...].astype(F32) + b[...].astype(F32)).astype(BF16)


def join_kernel(keep_ref, got_ref, out_ref):
    for j in range(out_ref.shape[0]):
        out_ref[j, 0:8] = keep_ref[8 * j : 8 * j + 8]
        out_ref[j, 8:16] = got_ref[8 * j : 8 * j + 8]


def levels_of(decay):
    n = decay.shape[1]
    parts = jnp.concatenate([t.astype(F32) for t in three_parts(decay)], axis=0).astype(BF16)
    upto = (iota((n, n), 0) >= iota((n, n), 1)).astype(BF16)
    before = (iota((n, n), 0) <= iota((n, n), 1)).astype(BF16)
    col = lax.dot_general(upto, parts, (((1,), (1,)), ((), ())), preferred_element_type=F32)
    row = dot(parts, before)
    return col[:, 0:2] + col[:, 2:4] + col[:, 4:6], row[0:2] + row[2:4] + row[4:6]


def inner_kernel(q_ref, k_ref, v_ref, decay_ref, inner_ref, state_ref, total_ref, send_ref):
    n = q_ref.shape[0]
    col, row = levels_of(decay_ref[...])
    causal = iota((n, n), 0) >= iota((n, n), 1)
    for h in range(2):
        cols = slice(h * 128, h * 128 + 128)
        q, k, v = q_ref[:, cols], k_ref[:, cols], v_ref[:, cols]
        scores = lax.dot_general(q, k, (((1,), (1,)), ((), ())), preferred_element_type=F32) * 128 ** (-0.5)
        spread = jnp.where(causal, col[:, h : h + 1] - row[h : h + 1], -jnp.inf)
        inner_ref[:, cols] = dot((scores * jnp.exp(spread)).astype(BF16), v)
        total = col[n - 1 : n, h : h + 1]
        scaled = (k.astype(F32) * jnp.exp(total - col[:, h : h + 1])).astype(BF16)
        state = dot_t(scaled, v)
        kept(h, (state, total), state_ref, total_ref)
        packed(h, (state, total), send_ref)


def rows_of_total(total, rows):
    a, b, c = (jnp.broadcast_to(t.astype(F32), (rows, 128)) for t in three_parts(total))
    r = iota((rows, 128), 0)
    return jnp.where(r == 0, a, jnp.where(r == 1, b, jnp.where(r == 2, c, 0.0))).astype(BF16)


def kept(h, run, state_ref, total_ref):
    state_ref[128 * h : 128 * h + 128] = run[0]
    total_ref[8 * h : 8 * h + 8] = jnp.broadcast_to(run[1], (8, 128))


def had(h, state_ref, total_ref):
    return state_ref[128 * h : 128 * h + 128], total_ref[8 * h : 8 * h + 1]


def packed(h, run, ref):
    ref[144 * h : 144 * h + 128] = run[0].astype(BF16)
    ref[144 * h + 128 : 144 * h + 144] = rows_of_total(run[1], 16)


def unpacked(h, ref):
    rows = ref[144 * h + 128 : 144 * h + 144].astype(F32)
    return ref[144 * h : 144 * h + 128].astype(F32), rows[0:1] + rows[1:2] + rows[2:3]


def after(earlier, later):
    return jnp.exp(later[1]) * earlier[0] + later[0], earlier[1] + later[1]


def chosen(which, a, b):
    return tuple(jnp.where(which, x, y) for x, y in zip(a, b))


def pair_kernel(state_ref, total_ref, got_ref, out_ref):
    first = lax.axis_index("c") == 0
    for h in range(2):
        mine, theirs = had(h, state_ref, total_ref), unpacked(h, got_ref)
        packed(h, after(chosen(first, mine, theirs), chosen(first, theirs, mine)), out_ref)


def row_kernel(own_ref, one_ref, two_ref, three_ref, before_ref, before_total_ref, out_ref):
    me = lax.axis_index("x")
    for h in range(2):
        pieces = [unpacked(h, r) for r in (own_ref, one_ref, two_ref, three_ref)]
        so_far = before = (jnp.zeros((128, 128), F32), jnp.zeros((1, 128), F32))
        for k in range(len(pieces)):
            before = chosen(me == k, so_far, before)
            back = lax.rem(me - k + len(pieces), len(pieces))
            here = pieces[0]
            for by in range(1, len(pieces)):
                here = chosen(back == by, pieces[by], here)
            so_far = after(so_far, here)
        kept(h, before, before_ref, before_total_ref)
        packed(h, so_far, out_ref)


def two_kernel(own_ref, one_ref, out_ref):
    for h in range(2):
        packed(h, after(unpacked(h, one_ref), unpacked(h, own_ref)), out_ref)


def four_kernel(own_ref, one_ref, two_ref, before_ref, before_total_ref, out_ref):
    for h in range(2):
        before = after(unpacked(h, two_ref), unpacked(h, one_ref))
        kept(h, before, before_ref, before_total_ref)
        packed(h, after(before, unpacked(h, own_ref)), out_ref)


def entering(h, four_ref, rows_ref, rows_total_ref, row_ref, row_total_ref, got_ref):
    before = after(after(unpacked(h, four_ref), had(h, rows_ref, rows_total_ref)), had(h, row_ref, row_total_ref))
    later = after(before, unpacked(h, got_ref))
    return jnp.where(lax.axis_index("c") == 0, before[0], later[0]).astype(BF16)


def mixer_kernel(q_ref, decay_ref, gain_ref, gate_ref, weight_ref, inner_ref, *refs):
    *refs, out_0, out_1, out_2, out_3, rows_ref = refs
    outs = (out_0, out_1, out_2, out_3)
    col, _ = levels_of(decay_ref[...])
    heads = []
    for h in range(2):
        cols = slice(h * 128, h * 128 + 128)
        carried = jnp.exp(col[:, h : h + 1]) * dot(q_ref[:, cols], entering(h, *refs))
        whole = inner_ref[:, cols] + carried
        normed = whole * lax.rsqrt(jnp.mean(whole * whole, axis=-1, keepdims=True) + epsilon) * gain_ref[h : h + 1]
        gate = gate_ref[:, cols].astype(F32)
        heads.append((normed * (gate * jax.nn.sigmoid(gate))).astype(BF16).astype(F32))
    rows_ref[...] = jnp.concatenate(heads, axis=1)
    part = outs[0].shape[0]
    rows = jnp.concatenate([rows_ref[span(k, part)] for k in range(len(outs))], axis=0)
    for lo in range(0, weight_ref.shape[1], 512):
        out = dot(rows.astype(BF16), weight_ref[:, lo : lo + 512]).astype(BF16)
        for k, ref in enumerate(outs):
            ref[:, lo : lo + 512] = out[k * part : (k + 1) * part]


def mix_sum_kernel(mine, right, far, left, out):
    out[...] = sum(r[...].astype(F32) for r in (mine, right, far, left)).astype(BF16)


def shifted(x, axis, by):
    n = lax.axis_size(axis)
    return lax.ppermute(x, axis, [(i, (i + by) % n) for i in range(n)])


def brought(x, axis, by):
    return lax.ppermute(x, axis, [(i, i + by) for i in range(lax.axis_size(axis) - by)])


def across_chips(x):
    n = lax.axis_size(ZX)
    out = lax.all_to_all(x.reshape(n, -1, x.shape[-1]), ZX, split_axis=0, concat_axis=0, tiled=True)
    return out.reshape(x.shape)


def experts(rows, gate, up, down):
    half, part = rows.shape[0] // 2, rows.shape[1]
    hidden = gate.shape[1]
    piece, sums = array((half, part), BF16), [array((2 * half, hidden), F32)] * 2
    top, low = rows[:half], rows[half:]
    left_a, right_b = shifted(top, "tp", 1), shifted(low, "tp", -1)
    left_b, right_a = shifted(low, "tp", 1), shifted(top, "tp", -1)
    far_a, far_b = shifted(left_a, "tp", 1), shifted(right_b, "tp", -1)
    rows_of, cols_of = (part, hidden), (hidden, part)
    g, u, far_gate, far_up, far_down, rest_down = call(
        near_kernel,
        sums + [array(rows_of, BF16)] * 2 + [array(cols_of, BF16), array((3, *cols_of), BF16)],
        rows,
        left_a,
        left_b,
        right_a,
        right_b,
        held=(gate, up, down),
        scratch_shapes=[pltpu.VMEM((3, *rows_of), BF16)] * 2 + [pltpu.SemaphoreType.DMA((12,))],
    )
    hid, to2a, to2b = call(
        far_kernel, [array((2 * half, hidden), BF16), piece, piece], far_a, far_b, g, u, far_gate, far_up, far_down
    )
    got_a, got_b = shifted(to2a, "tp", 1), shifted(to2b, "tp", -1)
    to1a, to1b, tom1a, tom1b, mine = call(rest_kernel, [piece] * 4 + [array((2 * half, part), BF16)], hid, rest_down)
    low_l, top_r = shifted(to1b, "tp", 1), shifted(tom1a, "tp", -1)
    to1a, tom1b = call(onward_kernel, [piece] * 2, to1a, tom1b, got_a, got_b)
    top_l, low_r = shifted(to1a, "tp", 1), shifted(tom1b, "tp", -1)
    return call(settle_kernel, array(rows.shape, BF16), mine, top_l, low_l, top_r, low_r)


def per_device(
    queries,
    key_rows,
    value_rows,
    out_gate,
    log_decay,
    head_gain,
    out_weight,
    moe_input,
    moe_gain,
    expert_gate,
    expert_up,
    expert_down,
    route_ids,
    route_weights,
):
    return layer(
        queries,
        key_rows,
        value_rows,
        out_gate,
        log_decay.T,
        head_gain,
        out_weight,
        moe_input,
        moe_gain.reshape(1, -1),
        expert_gate[0],
        expert_up[0],
        expert_down[0],
        route_ids.T,
        route_weights.T,
    )


def layer(q, k, v, out_gate, decay, head_gain, out_weight, x, gain, gate, up, down, ids, blend):
    tokens, width = x.shape
    part = width // lax.axis_size("tp")
    chips = lax.axis_size(ZX)
    capacity = 2 * ids.size // lax.axis_size(EP)
    rows = chips * capacity
    keep, send = call(
        functools.partial(dispatch_kernel, capacity), [array((rows, part), BF16)] * 2, ids, x, gain, plain=3
    )
    got = shifted(send, "c", 1)
    joined = call(join_kernel, array((chips, 2 * capacity, part), BF16), keep, got)
    arrived = across_chips(joined.reshape(-1, part))
    whole, state, total = array((288, 128), BF16), array((256, 128), F32), array((16, 128), F32)
    inner, own_state, own_total, state_send = call(
        inner_kernel, [array(q.shape, F32), state, total, whole], q, k, v, decay, plain=4
    )
    state_got = shifted(state_send, "c", 1)
    pair = call(pair_kernel, whole, own_state, own_total, state_got)
    around = [shifted(pair, "x", by) for by in (1, 2, 3)]
    row_before, row_total, row = call(row_kernel, [state, total, whole], pair, *around)
    one = brought(row, "z", 1)
    two = brought(call(two_kernel, whole, row, one), "z", 2)
    rows_before, rows_total, upto = call(four_kernel, [state, total, whole], row, one, two)
    mine, right, far, left = call(
        mixer_kernel,
        [array((q.shape[0] // 4, out_weight.shape[1]), BF16)] * 4,
        q,
        decay,
        head_gain,
        out_gate,
        out_weight,
        inner,
        brought(upto, "z", 4),
        rows_before,
        rows_total,
        row_before,
        row_total,
        state_got,
        loose=5,
        scratch_shapes=[pltpu.VMEM(q.shape, F32)],
    )
    mixer_out = call(
        mix_sum_kernel,
        jax.ShapeDtypeStruct(mine.shape, BF16),
        mine,
        shifted(right, "tp", 1),
        shifted(far, "tp", 2),
        shifted(left, "tp", 3),
    )
    weights = call(
        functools.partial(blend_weights_kernel, capacity), array((2, 2, rows, tokens), BF16), ids, blend, plain=2
    )
    results = experts(arrived, gate, up, down)
    back = across_chips(results).reshape(chips, 2 * capacity, part)
    sent = call(parted_kernel, array((rows, part), BF16), back)
    expert_out = call(
        blend_kernel,
        jax.ShapeDtypeStruct((tokens, part), BF16),
        weights,
        call(kept_blend_kernel, array((tokens, part), F32), weights, back),
        shifted(sent, "c", 1),
    )
    return mixer_out, expert_out


def solution(mesh):
    split = Mesh(mesh.devices.reshape(8, 4, 2, mesh.shape["tp"]), ("z", "x", "c", "tp"))
    return jax.shard_map(
        per_device,
        mesh=split,
        in_specs=(
            P(EP, "tp"),
            P(EP, "tp"),
            P(EP, "tp"),
            P(EP, "tp"),
            P(EP, "tp"),
            P("tp", None),
            P("tp", None),
            P(EP, None),
            P(),
            P(EP, None, "tp"),
            P(EP, None, "tp"),
            P(EP, "tp", None),
            P(EP, None),
            P(EP, None),
        ),
        out_specs=(P((*EP, "tp"), None), P(EP, "tp")),
        check_vma=False,
    )
```

```python
import functools

import jax
import jax.numpy as jnp
from jax import lax
from jax.experimental import pallas as pl
from jax.experimental.pallas import tpu as pltpu
from jax.sharding import Mesh
from jax.sharding import PartitionSpec as P


EP = ("z", "x", "c")
ZX = ("z", "x")
F32 = jnp.float32
BF16 = jnp.bfloat16
epsilon = 1e-06
VMEM_LIMIT = 16 << 20


def iota(shape, dim):
    return lax.broadcasted_iota(jnp.int32, shape, dim)


def dot(a, b):
    return jnp.dot(a, b, preferred_element_type=F32)


def dot_t(a, b):
    return lax.dot_general(a, b, (((0,), (0,)), ((), ())), preferred_element_type=F32)


def three_parts(x):
    a = x.astype(BF16)
    rest = x - a.astype(F32)
    b = rest.astype(BF16)
    return a, b, (rest - b.astype(F32)).astype(BF16)


def call(body, outs, *args, plain=0, loose=0, held=(), scratch_shapes=()):
    space = pl.BlockSpec(memory_space=pltpu.VMEM)
    kernel = pl.pallas_call(
        body,
        out_shape=outs,
        in_specs=[pl.BlockSpec(memory_space=pl.ANY)] * len(held) + [space] * len(args),
        out_specs=[space] * len(outs) if isinstance(outs, list) else space,
        scratch_shapes=scratch_shapes,
        compiler_params=pltpu.CompilerParams(vmem_limit_bytes=VMEM_LIMIT),
    )
    hbm = [pltpu.with_memory_space_constraint(a, pltpu.HBM) for a in (*held, *args[:plain])]
    rest = (pltpu.with_memory_space_constraint(a, pltpu.VMEM) for a in args[plain + loose :])
    return kernel(*hbm, *args[plain : plain + loose], *rest)


def array(shape, dtype):
    return pltpu.VMEM(shape, dtype)


def slot_members(ids_ref, half, rows, capacity):
    tokens = ids_ref.shape[1]
    core = lax.axis_index("c")
    slot = iota((rows, 1), 0)
    expert = (slot // capacity) * 2 + (core + half - 2 * core * half)
    first, second = ids_ref[0:1] == expert, ids_ref[1:2] == expert
    member = jnp.where(first | second, 1.0, 0.0)
    earlier = (iota((tokens, tokens), 0) < iota((tokens, tokens), 1)).astype(BF16)
    here = dot(member.astype(BF16), earlier).astype(jnp.int32) == slot % capacity
    return first & here, second & here


def dispatch_kernel(capacity, ids_ref, x_ref, gain_ref, send_ref, normed_ref):
    part = send_ref.shape[1]
    x = x_ref[...].astype(F32)
    scale = lax.rsqrt(jnp.mean(x * x, axis=-1, keepdims=True) + epsilon)
    cols = pl.ds(pl.multiple_of(lax.axis_index("tp") * part, part), part)
    normed = (x_ref[:, cols].astype(F32) * scale * gain_ref[:, cols]).astype(BF16)
    normed_ref[...] = normed
    slotted(capacity, ids_ref, 1, normed, send_ref)


def keep_kernel(capacity, ids_ref, normed_ref, keep_ref):
    slotted(capacity, ids_ref, 0, normed_ref[...], keep_ref)


def slotted(capacity, ids_ref, half, normed, out_ref):
    first, second = slot_members(ids_ref, half, out_ref.shape[0], capacity)
    hot = jnp.where(first | second, 1.0, 0.0).astype(BF16)
    out_ref[...] = dot(hot, normed).astype(BF16)


def blend_weights_kernel(capacity, ids_ref, w_ref, out_ref):
    for half in range(2):
        first, second = slot_members(ids_ref, half, out_ref.shape[2], capacity)
        blend = jnp.where(first, w_ref[0:1], 0.0) + jnp.where(second, w_ref[1:2], 0.0)
        hi = blend.astype(BF16)
        out_ref[half, 0] = hi
        out_ref[half, 1] = (blend - hi.astype(F32)).astype(BF16)


def blended(w_ref, half, rows):
    return dot_t(w_ref[half, 0], rows) + dot_t(w_ref[half, 1], rows)


def kept_blend_kernel(w_ref, back_ref, out_ref):
    keep = jnp.concatenate([back_ref[j, 0:8] for j in range(back_ref.shape[0])], axis=0)
    out_ref[...] = blended(w_ref, 0, keep)


def blend_kernel(w_ref, kept_ref, sent_ref, out_ref):
    out_ref[...] = (kept_ref[...] + blended(w_ref, 1, sent_ref[...])).astype(BF16)


def parted_kernel(back_ref, out_ref):
    for j in range(back_ref.shape[0]):
        out_ref[8 * j : 8 * j + 8] = back_ref[j, 8:16]


def span(k, size):
    n = lax.axis_size("tp")
    return pl.ds(pl.multiple_of(lax.rem(lax.axis_index("tp") + k, n) * size, size), size)


def tiles(size):
    return [slice(lo, min(size, lo + 256)) for lo in range(0, size, 256)]


def started(sems, *pairs):
    copies = [pltpu.make_async_copy(src, dst, sems.at[i]) for i, (src, dst) in enumerate(pairs)]
    for copy in copies:
        copy.start()
    return copies


def near_kernel(gate, up, down, own, left_a, left_b, right_a, right_b, g_ref, u_ref, far_gate, far_up, far_down, rest_down, gates, ups, sems):
    part = own.shape[1]
    left = (left_a, left_b)
    right = (right_a, right_b)
    order = ((0, (own,)), (3, left), (1, right))
    copies = started(
        sems,
        *(
            pair
            for i, (k, _) in enumerate(order)
            for pair in ((gate.at[span(k, part)], gates.at[i]), (up.at[span(k, part)], ups.at[i]))
        ),
        (gate.at[span(2, part)], far_gate),
        (up.at[span(2, part)], far_up),
        (down.at[:, span(2, part)], far_down),
        *((down.at[:, span(k, part)], rest_down.at[i]) for i, k in enumerate((1, 3, 0))),
    )
    for i, (_, refs) in enumerate(order):
        x = jnp.concatenate([r[...] for r in refs], axis=0)
        for weights, total, copy in ((gates, g_ref, copies[2 * i]), (ups, u_ref, copies[2 * i + 1])):
            copy.wait()
            for cols in tiles(total.shape[1]):
                new = dot(x, weights[i, :, cols])
                total[:, cols] = new if i == 0 else total[:, cols] + new
    for copy in copies[6:]:
        copy.wait()


def far_kernel(far_a, far_b, g_in, u_in, gate, up, down, hid_ref, to2a, to2b):
    half = far_a.shape[0]
    far = jnp.concatenate([far_a[...], far_b[...]], axis=0)
    for cols in tiles(gate.shape[1]):
        g = g_in[:, cols] + dot(far, gate[:, cols])
        u = u_in[:, cols] + dot(far, up[:, cols])
        hid_ref[:, cols] = (g * jax.nn.sigmoid(g) * u).astype(BF16)
    out = dot(hid_ref[...], down[...]).astype(BF16)
    to2a[...] = out[:half]
    to2b[...] = out[half:]


def rest_kernel(hid, down, to1a, to1b, tom1a, tom1b, mine):
    half = to1a.shape[0]
    for i, pair in enumerate(((to1a, to1b), (tom1a, tom1b), (mine.at[:half], mine.at[half:]))):
        out = dot(hid[...], down[i]).astype(BF16)
        for ref, rows in zip(pair, (out[:half], out[half:])):
            ref[...] = rows


def onward_kernel(to1a, tom1b, got_a, got_b, out1, outm1):
    out1[...] = (to1a[...].astype(F32) + got_a[...].astype(F32)).astype(BF16)
    outm1[...] = (tom1b[...].astype(F32) + got_b[...].astype(F32)).astype(BF16)


def settle_kernel(mine, top_l, low_l, top_r, low_r, out):
    half = top_l.shape[0]
    for rows, a, b in ((slice(0, half), top_l, top_r), (slice(half, 2 * half), low_l, low_r)):
        out[rows] = (mine[rows].astype(F32) + a[...].astype(F32) + b[...].astype(F32)).astype(BF16)


def join_kernel(keep_ref, got_ref, out_ref):
    for j in range(out_ref.shape[0]):
        out_ref[j, 0:8] = keep_ref[8 * j : 8 * j + 8]
        out_ref[j, 8:16] = got_ref[8 * j : 8 * j + 8]


def levels_of(decay):
    n = decay.shape[1]
    parts = jnp.concatenate([t.astype(F32) for t in three_parts(decay)], axis=0).astype(BF16)
    upto = (iota((n, n), 0) >= iota((n, n), 1)).astype(BF16)
    before = (iota((n, n), 0) <= iota((n, n), 1)).astype(BF16)
    col = lax.dot_general(upto, parts, (((1,), (1,)), ((), ())), preferred_element_type=F32)
    row = dot(parts, before)
    return col[:, 0:2] + col[:, 2:4] + col[:, 4:6], row[0:2] + row[2:4] + row[4:6]


def inner_kernel(q_ref, k_ref, v_ref, decay_ref, inner_ref, state_ref, total_ref, send_ref):
    n = q_ref.shape[0]
    col, row = levels_of(decay_ref[...])
    causal = iota((n, n), 0) >= iota((n, n), 1)
    for h in range(2):
        cols = slice(h * 128, h * 128 + 128)
        q, k, v = q_ref[:, cols], k_ref[:, cols], v_ref[:, cols]
        scores = lax.dot_general(q, k, (((1,), (1,)), ((), ())), preferred_element_type=F32) * 128 ** (-0.5)
        spread = jnp.where(causal, col[:, h : h + 1] - row[h : h + 1], -jnp.inf)
        inner_ref[:, cols] = dot((scores * jnp.exp(spread)).astype(BF16), v)
        total = col[n - 1 : n, h : h + 1]
        scaled = (k.astype(F32) * jnp.exp(total - col[:, h : h + 1])).astype(BF16)
        state = dot_t(scaled, v)
        kept(h, (state, total), state_ref, total_ref)
        packed(h, (state, total), send_ref)


def rows_of_total(total, rows):
    a, b, c = (jnp.broadcast_to(t.astype(F32), (rows, 128)) for t in three_parts(total))
    r = iota((rows, 128), 0)
    return jnp.where(r == 0, a, jnp.where(r == 1, b, jnp.where(r == 2, c, 0.0))).astype(BF16)


def kept(h, run, state_ref, total_ref):
    state_ref[128 * h : 128 * h + 128] = run[0]
    total_ref[8 * h : 8 * h + 8] = jnp.broadcast_to(run[1], (8, 128))


def had(h, state_ref, total_ref):
    return state_ref[128 * h : 128 * h + 128], total_ref[8 * h : 8 * h + 1]


def packed(h, run, ref):
    ref[144 * h : 144 * h + 128] = run[0].astype(BF16)
    ref[144 * h + 128 : 144 * h + 144] = rows_of_total(run[1], 16)


def unpacked(h, ref):
    rows = ref[144 * h + 128 : 144 * h + 144].astype(F32)
    return ref[144 * h : 144 * h + 128].astype(F32), rows[0:1] + rows[1:2] + rows[2:3]


def after(earlier, later):
    return jnp.exp(later[1]) * earlier[0] + later[0], earlier[1] + later[1]


def chosen(which, a, b):
    return tuple(jnp.where(which, x, y) for x, y in zip(a, b))


def pair_kernel(state_ref, total_ref, got_ref, out_ref):
    first = lax.axis_index("c") == 0
    for h in range(2):
        mine, theirs = had(h, state_ref, total_ref), unpacked(h, got_ref)
        packed(h, after(chosen(first, mine, theirs), chosen(first, theirs, mine)), out_ref)


def row_kernel(own_ref, one_ref, two_ref, three_ref, before_ref, before_total_ref, out_ref):
    me = lax.axis_index("x")
    for h in range(2):
        pieces = [unpacked(h, r) for r in (own_ref, one_ref, two_ref, three_ref)]
        so_far = before = (jnp.zeros((128, 128), F32), jnp.zeros((1, 128), F32))
        for k in range(len(pieces)):
            before = chosen(me == k, so_far, before)
            back = lax.rem(me - k + len(pieces), len(pieces))
            here = pieces[0]
            for by in range(1, len(pieces)):
                here = chosen(back == by, pieces[by], here)
            so_far = after(so_far, here)
        kept(h, before, before_ref, before_total_ref)
        packed(h, so_far, out_ref)


def two_kernel(own_ref, one_ref, out_ref):
    for h in range(2):
        packed(h, after(unpacked(h, one_ref), unpacked(h, own_ref)), out_ref)


def four_kernel(own_ref, one_ref, two_ref, before_ref, before_total_ref, out_ref):
    for h in range(2):
        before = after(unpacked(h, two_ref), unpacked(h, one_ref))
        kept(h, before, before_ref, before_total_ref)
        packed(h, after(before, unpacked(h, own_ref)), out_ref)


def entering(h, four_ref, rows_ref, rows_total_ref, row_ref, row_total_ref, got_ref):
    before = after(after(unpacked(h, four_ref), had(h, rows_ref, rows_total_ref)), had(h, row_ref, row_total_ref))
    later = after(before, unpacked(h, got_ref))
    return jnp.where(lax.axis_index("c") == 0, before[0], later[0]).astype(BF16)


def mixer_kernel(q_ref, decay_ref, gain_ref, gate_ref, weight_ref, inner_ref, *refs):
    *refs, out_0, out_1, out_2, out_3, rows_ref = refs
    outs = (out_0, out_1, out_2, out_3)
    col, _ = levels_of(decay_ref[...])
    heads = []
    for h in range(2):
        cols = slice(h * 128, h * 128 + 128)
        carried = jnp.exp(col[:, h : h + 1]) * dot(q_ref[:, cols], entering(h, *refs))
        whole = inner_ref[:, cols] + carried
        normed = whole * lax.rsqrt(jnp.mean(whole * whole, axis=-1, keepdims=True) + epsilon) * gain_ref[h : h + 1]
        gate = gate_ref[:, cols].astype(F32)
        heads.append((normed * (gate * jax.nn.sigmoid(gate))).astype(BF16).astype(F32))
    rows_ref[...] = jnp.concatenate(heads, axis=1)
    part = outs[0].shape[0]
    rows = jnp.concatenate([rows_ref[span(k, part)] for k in range(len(outs))], axis=0)
    for lo in range(0, weight_ref.shape[1], 512):
        out = dot(rows.astype(BF16), weight_ref[:, lo : lo + 512]).astype(BF16)
        for k, ref in enumerate(outs):
            ref[:, lo : lo + 512] = out[k * part : (k + 1) * part]


def mix_sum_kernel(mine, right, far, left, out):
    out[...] = sum(r[...].astype(F32) for r in (mine, right, far, left)).astype(BF16)


def shifted(x, axis, by):
    n = lax.axis_size(axis)
    return lax.ppermute(x, axis, [(i, (i + by) % n) for i in range(n)])


def brought(x, axis, by):
    return lax.ppermute(x, axis, [(i, i + by) for i in range(lax.axis_size(axis) - by)])


def across_chips(x):
    n = lax.axis_size(ZX)
    out = lax.all_to_all(x.reshape(n, -1, x.shape[-1]), ZX, split_axis=0, concat_axis=0, tiled=True)
    return out.reshape(x.shape)


def experts(rows, gate, up, down):
    half, part = rows.shape[0] // 2, rows.shape[1]
    hidden = gate.shape[1]
    piece, sums = array((half, part), BF16), [array((2 * half, hidden), F32)] * 2
    top, low = rows[:half], rows[half:]
    left_a, right_b = shifted(top, "tp", 1), shifted(low, "tp", -1)
    left_b, right_a = shifted(low, "tp", 1), shifted(top, "tp", -1)
    far_a, far_b = shifted(left_a, "tp", 1), shifted(right_b, "tp", -1)
    rows_of, cols_of = (part, hidden), (hidden, part)
    g, u, far_gate, far_up, far_down, rest_down = call(
        near_kernel,
        sums + [array(rows_of, BF16)] * 2 + [array(cols_of, BF16), array((3, *cols_of), BF16)],
        rows,
        left_a,
        left_b,
        right_a,
        right_b,
        held=(gate, up, down),
        scratch_shapes=[pltpu.VMEM((3, *rows_of), BF16)] * 2 + [pltpu.SemaphoreType.DMA((12,))],
    )
    hid, to2a, to2b = call(
        far_kernel, [array((2 * half, hidden), BF16), piece, piece], far_a, far_b, g, u, far_gate, far_up, far_down
    )
    got_a, got_b = shifted(to2a, "tp", 1), shifted(to2b, "tp", -1)
    to1a, to1b, tom1a, tom1b, mine = call(rest_kernel, [piece] * 4 + [array((2 * half, part), BF16)], hid, rest_down)
    low_l, top_r = shifted(to1b, "tp", 1), shifted(tom1a, "tp", -1)
    to1a, tom1b = call(onward_kernel, [piece] * 2, to1a, tom1b, got_a, got_b)
    top_l, low_r = shifted(to1a, "tp", 1), shifted(tom1b, "tp", -1)
    return call(settle_kernel, array(rows.shape, BF16), mine, top_l, low_l, top_r, low_r)


def per_device(
    queries,
    key_rows,
    value_rows,
    out_gate,
    log_decay,
    head_gain,
    out_weight,
    moe_input,
    moe_gain,
    expert_gate,
    expert_up,
    expert_down,
    route_ids,
    route_weights,
):
    return layer(
        queries,
        key_rows,
        value_rows,
        out_gate,
        log_decay.T,
        head_gain,
        out_weight,
        moe_input,
        moe_gain.reshape(1, -1),
        expert_gate[0],
        expert_up[0],
        expert_down[0],
        route_ids.T,
        route_weights.T,
    )


def layer(q, k, v, out_gate, decay, head_gain, out_weight, x, gain, gate, up, down, ids, blend):
    tokens, width = x.shape
    part = width // lax.axis_size("tp")
    chips = lax.axis_size(ZX)
    capacity = 2 * ids.size // lax.axis_size(EP)
    rows = chips * capacity
    slots = array((rows, part), BF16)
    send, normed = call(
        functools.partial(dispatch_kernel, capacity), [slots, array((tokens, part), BF16)], ids, x, gain, plain=3
    )
    keep = call(functools.partial(keep_kernel, capacity), slots, ids, normed, plain=1)
    got = shifted(send, "c", 1)
    joined = call(join_kernel, array((chips, 2 * capacity, part), BF16), keep, got)
    arrived = across_chips(joined.reshape(-1, part))
    whole, state, total = array((288, 128), BF16), array((256, 128), F32), array((16, 128), F32)
    inner, own_state, own_total, state_send = call(
        inner_kernel, [array(q.shape, F32), state, total, whole], q, k, v, decay, plain=4
    )
    state_got = shifted(state_send, "c", 1)
    pair = call(pair_kernel, whole, own_state, own_total, state_got)
    around = [shifted(pair, "x", by) for by in (1, 2, 3)]
    row_before, row_total, row = call(row_kernel, [state, total, whole], pair, *around)
    one = brought(row, "z", 1)
    two = brought(call(two_kernel, whole, row, one), "z", 2)
    rows_before, rows_total, upto = call(four_kernel, [state, total, whole], row, one, two)
    mine, right, far, left = call(
        mixer_kernel,
        [array((q.shape[0] // 4, out_weight.shape[1]), BF16)] * 4,
        q,
        decay,
        head_gain,
        out_gate,
        out_weight,
        inner,
        brought(upto, "z", 4),
        rows_before,
        rows_total,
        row_before,
        row_total,
        state_got,
        loose=5,
        scratch_shapes=[pltpu.VMEM(q.shape, F32)],
    )
    mixer_out = call(
        mix_sum_kernel,
        jax.ShapeDtypeStruct(mine.shape, BF16),
        mine,
        shifted(right, "tp", 1),
        shifted(far, "tp", 2),
        shifted(left, "tp", 3),
    )
    weights = call(
        functools.partial(blend_weights_kernel, capacity), array((2, 2, rows, tokens), BF16), ids, blend, plain=2
    )
    results = experts(arrived, gate, up, down)
    back = across_chips(results).reshape(chips, 2 * capacity, part)
    sent = call(parted_kernel, array((rows, part), BF16), back)
    expert_out = call(
        blend_kernel,
        jax.ShapeDtypeStruct((tokens, part), BF16),
        weights,
        call(kept_blend_kernel, array((tokens, part), F32), weights, back),
        shifted(sent, "c", 1),
    )
    return mixer_out, expert_out


def solution(mesh):
    split = Mesh(mesh.devices.reshape(8, 4, 2, mesh.shape["tp"]), ("z", "x", "c", "tp"))
    return jax.shard_map(
        per_device,
        mesh=split,
        in_specs=(
            P(EP, "tp"),
            P(EP, "tp"),
            P(EP, "tp"),
            P(EP, "tp"),
            P(EP, "tp"),
            P("tp", None),
            P("tp", None),
            P(EP, None),
            P(),
            P(EP, None, "tp"),
            P(EP, None, "tp"),
            P(EP, "tp", None),
            P(EP, None),
            P(EP, None),
        ),
        out_specs=(P((*EP, "tp"), None), P(EP, "tp")),
        check_vma=False,
    )
```
